512 devices in a mesh: fs: 64 (over z, y), tp: 8 (over x, core).
Axes of the slice: x: 4, y: 8, z: 8, core: 2. Of those that a mesh axis runs over, the one named last changes fastest.
Arguments:
- sequence_entries: bfloat16 [16384, 2048], P('fs', 'tp'), may hold values from -6 to 6
- former_norm_factor: float32 [2048], replicated, may hold values from 0.1 to 1.9
- conveyor_matrix: float32 [2048, 1536], P('fs', 'tp'), may hold values from -0.125 to 0.125
- conveyor_rescalers: float32 [1536], P('tp'), may hold values from 0.3 to 3
- blend_value_matrix: float32 [2048, 1536], P('fs', 'tp'), may hold values from -0.125 to 0.125
- blend_rescalers: float32 [1536], P('tp'), may hold values from 0.18 to 4.8, as said below
- blend_norm_factor: float32 [1536], P('tp'), may hold values from 0.1 to 1.9
- location_matrices: bfloat16 [24, 128, 128], P('tp'), may hold values from -0.5 to 0.5
- location_offsets: float32 [24, 128], P('tp'), may hold values from 0.1 to 1.9
- branch_emission_matrix: float32 [1536, 2048], P('tp', 'fs'), may hold values from -0.15625 to 0.15625
- emission_rescalers: float32 [2048], P('fs'), may hold values from 0.3 to 3
- latter_norm_factor: float32 [2048], replicated, may hold values from 0.1 to 1.9
- valve_matrix: float32 [2048, 5632], P('fs', 'tp'), may hold values from -0.125 to 0.125
- valve_rescalers: float32 [5632], P('tp'), may hold values from 0.3 to 3
- raising_matrix: float32 [2048, 5632], P('fs', 'tp'), may hold values from -0.125 to 0.125
- raising_rescalers: float32 [5632], P('tp'), may hold values from 0.3 to 3
- lowering_matrix: float32 [5632, 2048], P('tp', 'fs'), may hold values from -0.078125 to 0.078125
- lowering_rescalers: float32 [2048], P('fs'), may hold values from 0.3 to 3
Outputs:
- layer_out: bfloat16 [16384, 2048], P('fs', 'tp')
The draws below stay inside these ranges and needn't reach their ends.
Inputs may be any that keep to these rules, and one draw needn't show every extreme that they name: `blend_rescalers`: positive column scales.
All inputs are finite; a program needn't handle non-finite values.
Results may differ from the reference program's by a relative error of at most 0.02.
Values may be sent and summed in bfloat16 or wider, within the bound.
No kernel may reach another device: no remote copies, remote signals or barrier semaphores. Data moves between devices by JAX's collectives and lax.ppermute only.
A program may use at most 64 MiB of HBM per device.

```python
import math
import jax
import jax.numpy as jnp
from jax import lax

MODEL_BREADTH = 2048
FILTER_BUNDLES = 24
BUNDLE_BREADTH = 64
BLEND_BREADTH = 1536
FF = 5632
BLOCK = 128
WORD_TOTALITY = 16384
N_TP = 8


def draw_blend_rescalers(key, part):
    noise_key = jax.random.fold_in(key, 11)
    place = jnp.arange(BLEND_BREADTH, dtype=jnp.float32) / max(BLEND_BREADTH - 1, 1)
    jitter = jnp.exp(jax.random.uniform(noise_key, (BLEND_BREADTH,), jnp.float32, math.log(0.6), math.log(1.6)))
    ramp = jnp.exp(math.log(0.4) + place * math.log(5.0))
    return (ramp * jitter).astype(jnp.float32)


def shard_levels(key, shape, split, least, high):
    level, own = 1.0, jax.random.fold_in(key, 6)
    for axis_at, parts in split:
        heights = jnp.exp(jax.random.uniform(jax.random.fold_in(own, axis_at), (parts,), jnp.float32, least / len(split), high / len(split)))
        level = level * jnp.repeat(heights, shape[axis_at] // parts).reshape([-1 if axis == axis_at else 1 for axis in range(len(shape))])
    return level


def scatter_about(stream_key, extent, deviation, most, shards=(), kind=jnp.bfloat16):
    array = jax.random.normal(stream_key, extent, jnp.float32) * deviation
    if len(shards) > 0:
        array = shard_levels(stream_key, extent, shards, -0.22, 0.18) * array
    return jnp.clip(array, min=-most, max=most).astype(kind)


def setup_inputs(seed: int = 0) -> dict:
    key_of = jax.random.split(jax.random.key(seed), 19)
    sequence_entries = scatter_about(key_of[0], (WORD_TOTALITY, MODEL_BREADTH), 1.0, 6.0, ((0, 64), (1, 8)))
    former_norm_factor = jnp.clip(1.0 + 0.18 * jax.random.normal(key_of[1], (MODEL_BREADTH,), jnp.float32), 0.1, 1.9)
    conveyor_matrix = scatter_about(key_of[2], (MODEL_BREADTH, BLEND_BREADTH), MODEL_BREADTH ** -0.5, 0.125, ((0, 64), (1, 8)), jnp.float32)
    conveyor_rescalers = jnp.clip(jnp.exp(math.log(3.0) - 2.3025851 * jax.random.uniform(key_of[3], (BLEND_BREADTH,), jnp.float32) ** shard_levels(key_of[3], (BLEND_BREADTH,), ((0, 8),), -0.2, 0.2)), 0.3, 3.0)
    blend_value_matrix = scatter_about(key_of[4], (MODEL_BREADTH, BLEND_BREADTH), MODEL_BREADTH ** -0.5, 0.125, ((0, 64), (1, 8)), jnp.float32)
    blend_rescalers = draw_blend_rescalers(jax.random.fold_in(key_of[18], 71), 0)
    blend_norm_factor = jnp.clip(1.0 + 0.18 * jax.random.normal(key_of[6], (BLEND_BREADTH,), jnp.float32), 0.1, 1.9)
    location_matrices = scatter_about(key_of[7], (FILTER_BUNDLES, BLOCK, BLOCK), BLOCK ** -0.5, 0.5, ((0, 8),))
    location_offsets = jnp.clip(1.0 + 0.18 * jax.random.normal(key_of[8], (FILTER_BUNDLES, BLOCK), jnp.float32), 0.1, 1.9)
    branch_emission_matrix = scatter_about(key_of[9], (BLEND_BREADTH, MODEL_BREADTH), BLEND_BREADTH ** -0.5, 0.15625, ((0, 8), (1, 64)), jnp.float32)
    emission_rescalers = jnp.clip(jnp.exp(math.log(3.0) - 2.3025851 * jax.random.uniform(key_of[10], (MODEL_BREADTH,), jnp.float32) ** shard_levels(key_of[10], (MODEL_BREADTH,), ((0, 64),), -0.2, 0.2)), 0.3, 3.0)
    latter_norm_factor = jnp.clip(1.0 + 0.18 * jax.random.normal(key_of[11], (MODEL_BREADTH,), jnp.float32), 0.1, 1.9)
    valve_matrix = scatter_about(key_of[12], (MODEL_BREADTH, FF), MODEL_BREADTH ** -0.5, 0.125, ((0, 64), (1, 8)), jnp.float32)
    valve_rescalers = jnp.clip(jnp.exp(math.log(3.0) - 2.3025851 * jax.random.uniform(key_of[13], (FF,), jnp.float32) ** shard_levels(key_of[13], (FF,), ((0, 8),), -0.2, 0.2)), 0.3, 3.0)
    raising_matrix = scatter_about(key_of[14], (MODEL_BREADTH, FF), MODEL_BREADTH ** -0.5, 0.125, ((0, 64), (1, 8)), jnp.float32)
    raising_rescalers = jnp.clip(jnp.exp(math.log(3.0) - 2.3025851 * jax.random.uniform(key_of[15], (FF,), jnp.float32) ** shard_levels(key_of[15], (FF,), ((0, 8),), -0.2, 0.2)), 0.3, 3.0)
    lowering_matrix = scatter_about(key_of[16], (FF, MODEL_BREADTH), FF ** -0.5, 0.078125, ((0, 8), (1, 64)), jnp.float32)
    lowering_rescalers = jnp.clip(jnp.exp(math.log(3.0) - 2.3025851 * jax.random.uniform(key_of[17], (MODEL_BREADTH,), jnp.float32) ** shard_levels(key_of[17], (MODEL_BREADTH,), ((0, 64),), -0.2, 0.2)), 0.3, 3.0)
    return dict(sequence_entries=sequence_entries, former_norm_factor=former_norm_factor, conveyor_matrix=conveyor_matrix, conveyor_rescalers=conveyor_rescalers, blend_value_matrix=blend_value_matrix, blend_rescalers=blend_rescalers, blend_norm_factor=blend_norm_factor, location_matrices=location_matrices, location_offsets=location_offsets, branch_emission_matrix=branch_emission_matrix, emission_rescalers=emission_rescalers, latter_norm_factor=latter_norm_factor, valve_matrix=valve_matrix, valve_rescalers=valve_rescalers, raising_matrix=raising_matrix, raising_rescalers=raising_rescalers, lowering_matrix=lowering_matrix, lowering_rescalers=lowering_rescalers)


EPS = 1e-06

def normalize(rows, gain):
    values = rows.astype(jnp.float32)
    factor = lax.rsqrt(lax.optimization_barrier(jnp.mean(values * values, axis=-1, keepdims=True)) + EPS)
    return (values * factor * gain).astype(jnp.bfloat16)

def rescaled_matmul(left, weight, scale):
    return jnp.dot(left, weight.astype(jnp.bfloat16), preferred_element_type=jnp.float32) * scale

def split_sum(left, weight, scale, groups):
    width = left.shape[1] // groups
    total = jnp.zeros((left.shape[0], weight.shape[1]), jnp.float32)
    for index in range(groups):
        part_sum = rescaled_matmul(left[:, index * width:(index + 1) * width], weight[index * width:(index + 1) * width], scale).astype(jnp.bfloat16)
        part_sum = lax.optimization_barrier(part_sum)
        total = total + part_sum.astype(jnp.float32)
    return total

def reference(sequence_entries, former_norm_factor, conveyor_matrix, conveyor_rescalers, blend_value_matrix, blend_rescalers, blend_norm_factor, location_matrices, location_offsets, branch_emission_matrix, emission_rescalers, latter_norm_factor, valve_matrix, valve_rescalers, raising_matrix, raising_rescalers, lowering_matrix, lowering_rescalers):
    standardized_source = normalize(sequence_entries, former_norm_factor)
    conveyor_current = jax.nn.gelu(rescaled_matmul(standardized_source, conveyor_matrix, conveyor_rescalers))
    signal = jax.nn.gelu(rescaled_matmul(standardized_source, blend_value_matrix, blend_rescalers))
    factor = lax.rsqrt(lax.optimization_barrier(jnp.mean(signal * signal, axis=-1, keepdims=True)) + EPS)
    signal_norm = (signal * factor * blend_norm_factor).astype(jnp.bfloat16)
    lower_mask = jnp.tril(jnp.ones((BLOCK, BLOCK), bool))
    masked = jnp.where(lower_mask[None], location_matrices.astype(jnp.float32), jnp.float32(0.0))
    signal_blocks = signal_norm.astype(jnp.float32).reshape(WORD_TOTALITY // BLOCK, BLOCK, FILTER_BUNDLES, BUNDLE_BREADTH)
    location_blended = jnp.einsum('gts,bsgd->btgd', masked, signal_blocks) + location_offsets.T[None, :, :, None]
    filtered_result = (conveyor_current * location_blended.reshape(WORD_TOTALITY, FILTER_BUNDLES * BUNDLE_BREADTH)).astype(jnp.bfloat16)
    middle = (sequence_entries.astype(jnp.float32) + split_sum(filtered_result, branch_emission_matrix, emission_rescalers, N_TP)).astype(jnp.bfloat16)
    ffn_in = normalize(middle, latter_norm_factor)
    hidden = (jax.nn.silu(rescaled_matmul(ffn_in, valve_matrix, valve_rescalers)) * rescaled_matmul(ffn_in, raising_matrix, raising_rescalers)).astype(jnp.bfloat16)
    return (middle.astype(jnp.float32) + split_sum(hidden, lowering_matrix, lowering_rescalers, N_TP)).astype(jnp.bfloat16)
```

```python
import jax
import jax.numpy as jnp
from jax import lax
from jax.experimental import pallas as pl
from jax.experimental.pallas import tpu as pltpu
from jax.sharding import Mesh
from jax.sharding import PartitionSpec as P

FS = ("z", "y")
TP = ("x", "c")
EPS = 1e-06
BF = jnp.bfloat16
F32 = jnp.float32
NT = (((1,), (1,)), ((), ()))
VM = pl.BlockSpec(memory_space=pltpu.VMEM)
SM = pl.BlockSpec(memory_space=pltpu.SMEM)
ANY = pl.BlockSpec(memory_space=pl.ANY)


def from_everyone(x, axis):
    copies = jnp.broadcast_to(x, (lax.axis_size(axis), *x.shape))
    return lax.all_to_all(copies, axis, split_axis=0, concat_axis=0, tiled=True)


def gelu(v):
    return 0.5 * v * (1.0 + jnp.tanh(0.7978845608028654 * (v + 0.044715 * v * v * v)))


def project_kernel(order, x_ref, gain, scales, *refs):
    pieces, act_ref, sq_ref = refs[:8], refs[8], refs[9]
    total = jnp.zeros((256, 1), F32)
    for k in range(8):
        v = x_ref[k].astype(F32)
        total = total + jnp.sum(v * v, axis=1, keepdims=True)
    factor = lax.rsqrt(total / 2048.0 + EPS)
    prior = jnp.zeros((256, 384), F32)
    for d in range(8):
        k = order[d]
        rows = (x_ref[k].astype(F32) * factor * gain[k]).astype(BF)
        prior = prior + jnp.dot(rows, pieces[d][:, 0:384], preferred_element_type=F32)
    act = gelu(prior * scales[...])
    act_ref[...] = act
    signal = act[:, 192:384]
    ones = jnp.ones((8, 192), F32)
    sums = lax.dot_general(
        ones, signal * signal, NT, precision=lax.Precision.HIGHEST, preferred_element_type=F32
    )
    sq_ref[...] = sums[0:1]


def gate_kernel(order, act_ref, sq_ref, mats, offs, gain, *refs):
    pieces, out_ref, gated = refs[:8], refs[8], refs[9]
    total = jnp.sum(sq_ref[...], axis=0, keepdims=True)
    factor = lax.rsqrt(total / 1536.0 + EPS)
    rows = lax.broadcasted_iota(jnp.int32, (128, 128), 0)
    cols = lax.broadcasted_iota(jnp.int32, (128, 128), 1)
    lower = cols <= rows
    for g in range(3):
        mat = jnp.where(lower, mats[g].astype(F32), 0.0)
        for b in range(2):
            at = pl.ds(128 * b, 128)
            mix = (mat * factor[:, 128 * b : 128 * b + 128]).astype(BF)
            sig = (act_ref[at, 192 + 64 * g : 256 + 64 * g] * gain[:, 64 * g : 64 * g + 64]).astype(BF)
            mixed = jnp.dot(mix, sig, preferred_element_type=F32) + offs[:, g : g + 1]
            gated[at, 64 * g : 64 * g + 64] = (act_ref[at, 64 * g : 64 * g + 64] * mixed).astype(BF)
    left = gated[...]
    for d in range(8):
        part = lax.dot_general(left, pieces[d][:, 384:576], NT, preferred_element_type=F32)
        out_ref[0, order[d]] = part[0:128].astype(BF)
        out_ref[1, order[d]] = part[128:256].astype(BF)


def ffn_kernel(mid_ref, gain, w_ref, out_ref, w, acc, hid, sems):
    def fetch(k):
        return pltpu.make_async_copy(w_ref.at[k], w.at[k], sems.at[k])

    for k in range(8):
        fetch(k).start()
    total = jnp.zeros((128, 1), F32)
    for k in range(8):
        v = mid_ref[k].astype(F32)
        total = total + jnp.sum(v * v, axis=1, keepdims=True)
    factor = lax.rsqrt(total / 2048.0 + EPS)
    for k in range(8):
        rows = (mid_ref[k].astype(F32) * factor * gain[k]).astype(BF)
        fetch(k).wait()
        for c in range(2):
            piece = w[k, :, c, :, 0:1408].reshape(256, 1408)
            part = jnp.dot(rows, piece, preferred_element_type=F32)
            if k == 0:
                acc[c] = part
            else:
                acc[c] = acc[c] + part
    for c in range(2):
        g = acc[c, :, 0:640]
        u = acc[c, :, 640:1280]
        hid[c, :, 0:640] = (g * jax.nn.sigmoid(g) * u).astype(BF)
        g = acc[c, :, 1280:1344]
        u = acc[c, :, 1344:1408]
        hid[c, :, 640:704] = (g * jax.nn.sigmoid(g) * u).astype(BF)
    for k in range(8):
        part = jnp.zeros((128, 256), F32)
        for c in range(2):
            piece = w[k, :, c, :, 1408:2112].reshape(256, 704)
            part = part + lax.dot_general(hid[c], piece, NT, preferred_element_type=F32)
        out_ref[k] = part.astype(BF)


def on_device(
    sequence_entries,
    former_norm_factor,
    conveyor_matrix,
    conveyor_rescalers,
    blend_value_matrix,
    blend_rescalers,
    blend_norm_factor,
    location_matrices,
    location_offsets,
    branch_emission_matrix,
    emission_rescalers,
    latter_norm_factor,
    valve_matrix,
    valve_rescalers,
    raising_matrix,
    raising_rescalers,
    lowering_matrix,
    lowering_rescalers,
):
    z, x, c = lax.axis_index("z"), lax.axis_index("x"), lax.axis_index("c")
    swap = [(0, 1), (1, 0)]
    emission = (branch_emission_matrix * emission_rescalers).T.astype(BF)
    own = jnp.concatenate(
        [
            conveyor_matrix.astype(BF),
            blend_value_matrix.astype(BF),
            emission,
            jnp.zeros((32, 64), BF),
        ],
        axis=1,
    )
    gate = (valve_matrix * valve_rescalers).astype(BF)
    up = (raising_matrix * raising_rescalers).astype(BF)
    down = (lowering_matrix * lowering_rescalers).T.astype(BF)
    ffn_own = jnp.concatenate([gate[:, :640], up[:, :640], gate[:, 640:], up[:, 640:], down], axis=1)
    ffn_all = lax.all_gather(ffn_own, ("z", "y", "c"), axis=0, tiled=True)

    first = from_everyone(own, "y").reshape(256, 640)
    rows = from_everyone(sequence_entries, TP)
    pieces, order = [first], [z]
    ahead = behind = first
    for step in range(1, 5):
        ahead = lax.ppermute(ahead, "z", [(i, (i + 1) % 8) for i in range(8)])
        pieces.append(ahead)
        order.append((z - step) % 8)
        if step < 4:
            behind = lax.ppermute(behind, "z", [(i, (i - 1) % 8) for i in range(8)])
            pieces.append(behind)
            order.append((z + step) % 8)
    order = jnp.stack(order).astype(jnp.int32)

    act, own_sq = pl.pallas_call(
        project_kernel,
        in_specs=[SM] + [VM] * 11,
        out_specs=[VM, VM],
        out_shape=[jax.ShapeDtypeStruct((256, 384), F32), jax.ShapeDtypeStruct((1, 256), F32)],
        name="project",
    )(
        order,
        rows,
        former_norm_factor.reshape(8, 1, 256),
        jnp.concatenate([conveyor_rescalers, blend_rescalers]).reshape(1, 384),
        *pieces,
    )
    all_sq = lax.all_gather(own_sq, TP, axis=0, tiled=True)
    parts = pl.pallas_call(
        gate_kernel,
        in_specs=[SM] + [VM] * 13,
        out_specs=VM,
        out_shape=jax.ShapeDtypeStruct((2, 8, 128, 256), BF),
        scratch_shapes=[pltpu.VMEM((256, 192), BF)],
        name="gating",
    )(
        order,
        act,
        all_sq,
        location_matrices,
        location_offsets.T,
        blend_norm_factor.reshape(1, 192),
        *pieces,
    )
    kept = lax.dynamic_index_in_dim(parts, c, 0, keepdims=False)
    sent = lax.dynamic_index_in_dim(parts, 1 - c, 0, keepdims=False)
    got = lax.ppermute(sent, "c", swap)
    both = (kept.astype(F32) + got.astype(F32)).astype(BF).reshape(4, 2, 128, 256)
    shares = lax.all_to_all(both, "x", 0, 0, tiled=True)
    base = lax.dynamic_slice(rows, (2 * x, 128 * c, 0), (2, 128, 256))
    mid_own = (base.astype(F32) + jnp.sum(shares.astype(F32), axis=0)).astype(BF)
    mid = lax.all_gather(mid_own, "x", axis=0, tiled=True)
    outs = pl.pallas_call(
        ffn_kernel,
        in_specs=[VM, VM, ANY],
        out_specs=VM,
        out_shape=jax.ShapeDtypeStruct((8, 128, 256), BF),
        scratch_shapes=[
            pltpu.VMEM((8, 8, 2, 32, 2112), BF),
            pltpu.VMEM((2, 128, 1408), F32),
            pltpu.VMEM((2, 128, 704), BF),
            pltpu.SemaphoreType.DMA((8,)),
        ],
        name="ffn",
    )(mid, latter_norm_factor.reshape(8, 1, 256), ffn_all.reshape(8, 8, 2, 32, 2112))
    ffn_shares = lax.all_to_all(outs, TP, 0, 0, tiled=True).reshape(4, 2, 128, 256)
    mid_kept = lax.dynamic_index_in_dim(mid_own, c, 0, keepdims=False)
    mid_sent = lax.dynamic_index_in_dim(mid_own, 1 - c, 0, keepdims=False)
    mid_got = lax.ppermute(mid_sent, "c", swap)
    lower = jnp.where(c == 0, mid_kept, mid_got)
    upper = jnp.where(c == 0, mid_got, mid_kept)
    mid_here = jnp.stack([lower, upper])
    out = mid_here.astype(F32) + jnp.sum(ffn_shares.astype(F32), axis=0)
    return out.astype(BF).reshape(256, 256)


def solution(mesh):
    finer = Mesh(mesh.devices.reshape(8, 8, 4, 2), ("z", "y", "x", "c"))
    return jax.shard_map(
        on_device,
        mesh=finer,
        in_specs=(
            P(FS, TP),
            P(),
            P(FS, TP),
            P(TP),
            P(FS, TP),
            P(TP),
            P(TP),
            P(TP, None, None),
            P(TP, None),
            P(TP, FS),
            P(FS),
            P(),
            P(FS, TP),
            P(TP),
            P(FS, TP),
            P(TP),
            P(TP, FS),
            P(FS),
        ),
        out_specs=P(FS, TP),
        check_vma=False,
    )
```

```python
import jax
import jax.numpy as jnp
from jax import lax
from jax.experimental import pallas as pl
from jax.experimental.pallas import tpu as pltpu
from jax.sharding import Mesh
from jax.sharding import PartitionSpec as P

FS = ("z", "y")
TP = ("x", "c")
EPS = 1e-06
BF = jnp.bfloat16
F32 = jnp.float32
NT = (((1,), (1,)), ((), ()))
VM = pl.BlockSpec(memory_space=pltpu.VMEM)
SM = pl.BlockSpec(memory_space=pltpu.SMEM)
ANY = pl.BlockSpec(memory_space=pl.ANY)


def from_everyone(x, axis):
    copies = jnp.broadcast_to(x, (lax.axis_size(axis), *x.shape))
    return lax.all_to_all(copies, axis, split_axis=0, concat_axis=0, tiled=True)


def gelu(v):
    return 0.5 * v * (1.0 + jnp.tanh(0.7978845608028654 * (v + 0.044715 * v * v * v)))


def upright(row, n):
    same = lax.broadcasted_iota(jnp.int32, (n, n), 0) == lax.broadcasted_iota(jnp.int32, (n, n), 1)
    return jnp.sum(jnp.where(same, row.reshape(1, n), 0.0), axis=1, keepdims=True)


def pack_kernel(conv, blend, emis, emis_s, valve, valve_s, raising, raising_s, low, low_s, own, ffn):
    emission = emis[...] * upright(emis_s[...], 32)
    packed = jnp.concatenate([conv[...], blend[...], emission, jnp.zeros((32, 64), F32)], axis=1)
    packed = packed.astype(BF)
    for k in range(8):
        own[k] = packed
    gate = valve[...] * valve_s[...].reshape(1, 704)
    up = raising[...] * raising_s[...].reshape(1, 704)
    ffn[:, 0:640] = gate[:, 0:640].astype(BF)
    ffn[:, 640:1280] = up[:, 0:640].astype(BF)
    ffn[:, 1280:1408] = jnp.concatenate([gate[:, 640:704], up[:, 640:704]], axis=1).astype(BF)
    ffn[:, 1408:2112] = (low[...] * upright(low_s[...], 32)).astype(BF)


def spread(order, left, right):
    found = []
    for half, refs in enumerate((left, right)):
        place = 0
        for ref in refs:
            for k in range(ref.shape[0]):
                found.append((order[half, place], half, ref, k))
                place += 1
    return found


def project_kernel(order, x_ref, gain, conv_s, blend_s, *refs):
    pieces, act_ref, sq_ref = refs[:10], refs[10], refs[11]
    total = jnp.zeros((256, 1), F32)
    for k in range(8):
        v = x_ref[k].astype(F32)
        total = total + jnp.sum(v * v, axis=1, keepdims=True)
    factor = lax.rsqrt(total / 2048.0 + EPS)
    prior = jnp.zeros((256, 384), F32)
    for block, half, ref, k in spread(order, pieces[:5], pieces[5:]):
        cols = pl.ds(128 * half, 128)
        rows = (x_ref[block, :, cols].astype(F32) * factor * gain[block, :, cols]).astype(BF)
        prior = prior + jnp.dot(rows, ref[k, :, 0:384], preferred_element_type=F32)
    scales = jnp.concatenate([conv_s[...].reshape(1, 192), blend_s[...].reshape(1, 192)], axis=1)
    act = gelu(prior * scales)
    act_ref[...] = act
    signal = act[:, 192:384]
    ones = jnp.ones((8, 192), F32)
    sums = lax.dot_general(
        ones, signal * signal, NT, precision=lax.Precision.HIGHEST, preferred_element_type=F32
    )
    sq_ref[0] = sums[0:1]


def gate_kernel(order, core, act_ref, sq_ref, mats, offs, gain, *refs):
    pieces, kept, sent, gated = refs[:10], refs[10], refs[11], refs[12]
    total = jnp.sum(sq_ref[...], axis=0)
    factor = lax.rsqrt(total / 1536.0 + EPS)
    rows = lax.broadcasted_iota(jnp.int32, (128, 128), 0)
    cols = lax.broadcasted_iota(jnp.int32, (128, 128), 1)
    lower = cols <= rows
    gains = gain[...].reshape(1, 192)
    for g in range(3):
        mat = jnp.where(lower, mats[g].astype(F32), 0.0)
        for b in range(2):
            at = pl.ds(128 * b, 128)
            mix = (mat * factor[:, 128 * b : 128 * b + 128]).astype(BF)
            sig = (act_ref[at, 192 + 64 * g : 256 + 64 * g] * gains[:, 64 * g : 64 * g + 64]).astype(BF)
            mixed = jnp.dot(mix, sig, preferred_element_type=F32) + upright(offs[g], 128)
            gated[b, :, 64 * g : 64 * g + 64] = (
                act_ref[at, 64 * g : 64 * g + 64] * mixed
            ).astype(BF)
    here = core[0]
    mine, other = gated[here], gated[1 - here]
    for block, half, ref, k in spread(order, pieces[:5], pieces[5:]):
        piece = ref[k, :, 384:576]
        cols = pl.ds(128 * half, 128)
        part = lax.dot_general(mine, piece, NT, preferred_element_type=F32)
        kept[block, :, cols] = part.astype(BF)
        part = lax.dot_general(other, piece, NT, preferred_element_type=F32)
        sent[block, :, cols] = part.astype(BF)


def exchange(own, flip):
    to_pair = [(i, (((i + flip) ^ 1) - flip) % 8) for i in range(8)]
    to_next = [(i, (((i + 1 - flip) ^ 1) - 1 + flip) % 8) for i in range(8)]
    got = lax.ppermute(own, "z", to_pair)
    batch = jnp.concatenate([own, got])
    pieces = [own, got]
    for turn in (to_next, to_pair, to_next):
        batch = lax.ppermute(batch, "z", turn)
        pieces.append(batch)
    return pieces


def blocks(z):
    out = 2 * ((z + jnp.arange(2)) & 1) - 1
    steps = jnp.array([0, -1, 1, 2, -2, -3, 3, 4])
    return ((z + out[:, None] * steps) & 7).astype(jnp.int32)


def ffn_kernel(mid_ref, gain, w_ref, out_ref, w, acc, hid, sems):
    def fetch(k):
        return pltpu.make_async_copy(w_ref.at[k], w.at[k], sems.at[k])

    for k in range(8):
        fetch(k).start()
    total = jnp.zeros((128, 1), F32)
    for k in range(8):
        v = mid_ref[k].astype(F32)
        total = total + jnp.sum(v * v, axis=1, keepdims=True)
    factor = lax.rsqrt(total / 2048.0 + EPS)
    for k in range(8):
        rows = (mid_ref[k].astype(F32) * factor * gain[k]).astype(BF)
        fetch(k).wait()
        for c in range(2):
            piece = w[k, :, c, :, 0:1408].reshape(256, 1408)
            part = jnp.dot(rows, piece, preferred_element_type=F32)
            if k == 0:
                acc[c] = part
            else:
                acc[c] = acc[c] + part
    for c in range(2):
        g = acc[c, :, 0:640]
        u = acc[c, :, 640:1280]
        hid[c, :, 0:640] = (g * jax.nn.sigmoid(g) * u).astype(BF)
        g = acc[c, :, 1280:1344]
        u = acc[c, :, 1344:1408]
        hid[c, :, 640:704] = (g * jax.nn.sigmoid(g) * u).astype(BF)
    for k in range(8):
        part = jnp.zeros((128, 256), F32)
        for c in range(2):
            piece = w[k, :, c, :, 1408:2112].reshape(256, 704)
            part = part + lax.dot_general(hid[c], piece, NT, preferred_element_type=F32)
        out_ref[k] = part.astype(BF)


def on_device(
    sequence_entries,
    former_norm_factor,
    conveyor_matrix,
    conveyor_rescalers,
    blend_value_matrix,
    blend_rescalers,
    blend_norm_factor,
    location_matrices,
    location_offsets,
    branch_emission_matrix,
    emission_rescalers,
    latter_norm_factor,
    valve_matrix,
    valve_rescalers,
    raising_matrix,
    raising_rescalers,
    lowering_matrix,
    lowering_rescalers,
):
    z, x, c = lax.axis_index("z"), lax.axis_index("x"), lax.axis_index("c")
    swap = [(0, 1), (1, 0)]
    own, ffn_own = pl.pallas_call(
        pack_kernel,
        in_specs=[VM] * 10,
        out_specs=[VM, VM],
        out_shape=[jax.ShapeDtypeStruct((8, 32, 640), BF), jax.ShapeDtypeStruct((32, 2112), BF)],
        name="pack",
    )(
        conveyor_matrix,
        blend_value_matrix,
        branch_emission_matrix.T,
        emission_rescalers,
        valve_matrix,
        valve_rescalers,
        raising_matrix,
        raising_rescalers,
        lowering_matrix.T,
        lowering_rescalers,
    )
    ffn_all = lax.all_gather(ffn_own, ("z", "y", "c"), axis=0, tiled=True)

    first = lax.all_to_all(own, "y", 0, 0, tiled=True)
    rows = from_everyone(sequence_entries, TP)
    left = exchange(first[:4].reshape(1, 128, 640), 0)
    right = exchange(first[4:].reshape(1, 128, 640), 1)
    pieces = left + right
    order = blocks(z)

    act, own_sq = pl.pallas_call(
        project_kernel,
        in_specs=[SM] + [VM] * 14,
        out_specs=[VM, VM],
        out_shape=[jax.ShapeDtypeStruct((256, 384), F32), jax.ShapeDtypeStruct((1, 1, 256), F32)],
        name="project",
    )(
        order,
        rows,
        former_norm_factor.reshape(8, 1, 256),
        conveyor_rescalers,
        blend_rescalers,
        *pieces,
    )
    all_sq = lax.all_gather(own_sq, TP, axis=0, tiled=True)
    kept, sent = pl.pallas_call(
        gate_kernel,
        in_specs=[SM, SM] + [VM] * 15,
        out_specs=[VM, VM],
        out_shape=[jax.ShapeDtypeStruct((8, 128, 256), BF)] * 2,
        scratch_shapes=[pltpu.VMEM((2, 128, 192), BF)],
        name="gating",
    )(
        order,
        c.astype(jnp.int32).reshape(1),
        act,
        all_sq,
        location_matrices,
        location_offsets,
        blend_norm_factor,
        *pieces,
    )
    got = lax.ppermute(sent, "c", swap)
    both = (kept.astype(F32) + got.astype(F32)).astype(BF).reshape(4, 2, 128, 256)
    shares = lax.all_to_all(both, "x", 0, 0, tiled=True)
    base = lax.dynamic_slice(rows, (2 * x, 128 * c, 0), (2, 128, 256))
    mid_own = (base.astype(F32) + jnp.sum(shares.astype(F32), axis=0)).astype(BF)
    mid = lax.all_gather(mid_own, "x", axis=0, tiled=True)
    outs = pl.pallas_call(
        ffn_kernel,
        in_specs=[VM, VM, ANY],
        out_specs=VM,
        out_shape=jax.ShapeDtypeStruct((8, 128, 256), BF),
        scratch_shapes=[
            pltpu.VMEM((8, 8, 2, 32, 2112), BF),
            pltpu.VMEM((2, 128, 1408), F32),
            pltpu.VMEM((2, 128, 704), BF),
            pltpu.SemaphoreType.DMA((8,)),
        ],
        name="ffn",
    )(mid, latter_norm_factor.reshape(8, 1, 256), ffn_all.reshape(8, 8, 2, 32, 2112))
    ffn_shares = lax.all_to_all(outs, TP, 0, 0, tiled=True).reshape(4, 2, 128, 256)
    mid_kept = lax.dynamic_index_in_dim(mid_own, c, 0, keepdims=False)
    mid_sent = lax.dynamic_index_in_dim(mid_own, 1 - c, 0, keepdims=False)
    mid_got = lax.ppermute(mid_sent, "c", swap)
    lower = jnp.where(c == 0, mid_kept, mid_got)
    upper = jnp.where(c == 0, mid_got, mid_kept)
    mid_here = jnp.stack([lower, upper])
    out = mid_here.astype(F32) + jnp.sum(ffn_shares.astype(F32), axis=0)
    return out.astype(BF).reshape(256, 256)


def solution(mesh):
    finer = Mesh(mesh.devices.reshape(8, 8, 4, 2), ("z", "y", "x", "c"))
    return jax.shard_map(
        on_device,
        mesh=finer,
        in_specs=(
            P(FS, TP),
            P(),
            P(FS, TP),
            P(TP),
            P(FS, TP),
            P(TP),
            P(TP),
            P(TP, None, None),
            P(TP, None),
            P(TP, FS),
            P(FS),
            P(),
            P(FS, TP),
            P(TP),
            P(FS, TP),
            P(TP),
            P(TP, FS),
            P(FS),
        ),
        out_specs=P(FS, TP),
        check_vma=False,
    )
```

```python
import jax
import jax.numpy as jnp
from jax import lax
from jax.experimental import pallas as pl
from jax.experimental.pallas import tpu as pltpu
from jax.sharding import Mesh
from jax.sharding import PartitionSpec as P

FS = ("z", "y")
TP = ("x", "c")
EPS = 1e-06
BF = jnp.bfloat16
F32 = jnp.float32
NT = (((1,), (1,)), ((), ()))
VM = pl.BlockSpec(memory_space=pltpu.VMEM)
SM = pl.BlockSpec(memory_space=pltpu.SMEM)
ANY = pl.BlockSpec(memory_space=pl.ANY)


def from_everyone(x, axis):
    copies = jnp.broadcast_to(x, (lax.axis_size(axis), *x.shape))
    return lax.all_to_all(copies, axis, split_axis=0, concat_axis=0, tiled=True)


def gelu(v):
    return 0.5 * v * (1.0 + jnp.tanh(0.7978845608028654 * (v + 0.044715 * v * v * v)))


def upright(row, n):
    same = lax.broadcasted_iota(jnp.int32, (n, n), 0) == lax.broadcasted_iota(jnp.int32, (n, n), 1)
    return jnp.sum(jnp.where(same, row.reshape(1, n), 0.0), axis=1, keepdims=True)


def pack_kernel(conv, blend, emis, emis_s, valve, valve_s, raising, raising_s, low, low_s, seq, own, ffn, seqs):
    emission = emis[...] * upright(emis_s[...], 32)
    packed = jnp.concatenate([conv[...], blend[...], emission, jnp.zeros((32, 64), F32)], axis=1)
    packed = packed.astype(BF)
    for k in range(8):
        own[k] = packed
        seqs[k] = seq[...]
    gate = valve[...] * valve_s[...].reshape(1, 704)
    up = raising[...] * raising_s[...].reshape(1, 704)
    ffn[:, 0:640] = gate[:, 0:640].astype(BF)
    ffn[:, 640:1280] = up[:, 0:640].astype(BF)
    ffn[:, 1280:1408] = jnp.concatenate([gate[:, 640:704], up[:, 640:704]], axis=1).astype(BF)
    ffn[:, 1408:2112] = (low[...] * upright(low_s[...], 32)).astype(BF)


def spread(order, left, right, place=0):
    found = []
    for half, refs in enumerate((left, right)):
        at = place
        for ref in refs:
            for k in range(ref.shape[0]):
                found.append((order[half, at], half, ref, k))
                at += 1
    return found


def multiply(found, x_ref, gain, factor, prior):
    for block, half, ref, k in found:
        cols = pl.ds(128 * half, 128)
        rows = (x_ref[block, :, cols].astype(F32) * factor * gain[block, :, cols]).astype(BF)
        prior = prior + jnp.dot(rows, ref[k, :, 0:384], preferred_element_type=F32)
    return prior


def early_kernel(order, x_ref, gain, *refs):
    pieces, prior_ref, factor_ref = refs[:8], refs[8], refs[9]
    total = jnp.zeros((256, 1), F32)
    for k in range(8):
        v = x_ref[k].astype(F32)
        total = total + jnp.sum(v * v, axis=1, keepdims=True)
    factor = lax.rsqrt(total / 2048.0 + EPS)
    factor_ref[...] = jnp.broadcast_to(factor, (256, 128))
    found = spread(order, pieces[:4], pieces[4:])
    prior_ref[...] = multiply(found, x_ref, gain, factor, jnp.zeros((256, 384), F32))


def project_kernel(order, x_ref, gain, conv_s, blend_s, prior, factor, left, right, act_ref, sq_ref):
    found = spread(order, [left], [right], 6)
    prior = multiply(found, x_ref, gain, factor[:, 0:1], prior[...])
    scales = jnp.concatenate([conv_s[...].reshape(1, 192), blend_s[...].reshape(1, 192)], axis=1)
    act = gelu(prior * scales)
    act_ref[...] = act
    signal = act[:, 192:384]
    ones = jnp.ones((8, 192), F32)
    sums = lax.dot_general(
        ones, signal * signal, NT, precision=lax.Precision.HIGHEST, preferred_element_type=F32
    )
    sq_ref[0] = sums[0:1]


def gate_kernel(order, core, act_ref, sq_ref, mats, offs, gain, *refs):
    pieces, kept, sent, gated = refs[:10], refs[10], refs[11], refs[12]
    total = jnp.sum(sq_ref[...], axis=0)
    factor = lax.rsqrt(total / 1536.0 + EPS)
    rows = lax.broadcasted_iota(jnp.int32, (128, 128), 0)
    cols = lax.broadcasted_iota(jnp.int32, (128, 128), 1)
    lower = cols <= rows
    gains = gain[...].reshape(1, 192)
    for g in range(3):
        mat = jnp.where(lower, mats[g].astype(F32), 0.0)
        for b in range(2):
            at = pl.ds(128 * b, 128)
            mix = (mat * factor[:, 128 * b : 128 * b + 128]).astype(BF)
            sig = (act_ref[at, 192 + 64 * g : 256 + 64 * g] * gains[:, 64 * g : 64 * g + 64]).astype(BF)
            mixed = jnp.dot(mix, sig, preferred_element_type=F32) + upright(offs[g], 128)
            gated[b, :, 64 * g : 64 * g + 64] = (
                act_ref[at, 64 * g : 64 * g + 64] * mixed
            ).astype(BF)
    here = core[0]
    mine, other = gated[here], gated[1 - here]
    for block, half, ref, k in spread(order, pieces[:5], pieces[5:]):
        piece = ref[k, :, 384:576]
        cols = pl.ds(128 * half, 128)
        part = lax.dot_general(mine, piece, NT, preferred_element_type=F32)
        kept[block, :, cols] = part.astype(BF)
        part = lax.dot_general(other, piece, NT, preferred_element_type=F32)
        sent[block, :, cols] = part.astype(BF)


def exchange(own, flip):
    to_pair = [(i, (((i + flip) ^ 1) - flip) % 8) for i in range(8)]
    to_next = [(i, (((i + 1 - flip) ^ 1) - 1 + flip) % 8) for i in range(8)]
    got = lax.ppermute(own, "z", to_pair)
    batch = jnp.concatenate([own, got])
    pieces = [own, got]
    for turn in (to_next, to_pair, to_next):
        batch = lax.ppermute(batch, "z", turn)
        pieces.append(batch)
    return pieces


def blocks(z):
    out = 2 * ((z + jnp.arange(2)) & 1) - 1
    steps = jnp.array([0, -1, 1, 2, -2, -3, 3, 4])
    return ((z + out[:, None] * steps) & 7).astype(jnp.int32)


def ffn_kernel(mid_ref, gain, w_ref, out_ref, w, acc, hid, sems):
    def fetch(k, part):
        cols = pl.ds(1408 * part, 1408 - 704 * part)
        at = (k, slice(None), slice(None), slice(None), cols)
        return pltpu.make_async_copy(w_ref.at[at], w.at[at], sems.at[part, k])

    for part in range(2):
        for k in range(8):
            fetch(k, part).start()
    total = jnp.zeros((128, 1), F32)
    for k in range(8):
        v = mid_ref[k].astype(F32)
        total = total + jnp.sum(v * v, axis=1, keepdims=True)
    factor = lax.rsqrt(total / 2048.0 + EPS)
    for k in range(8):
        rows = (mid_ref[k].astype(F32) * factor * gain[k]).astype(BF)
        fetch(k, 0).wait()
        for c in range(2):
            piece = w[k, :, c, :, 0:1408].reshape(256, 1408)
            part = jnp.dot(rows, piece, preferred_element_type=F32)
            if k == 0:
                acc[c] = part
            else:
                acc[c] = acc[c] + part
    for c in range(2):
        g = acc[c, :, 0:640]
        u = acc[c, :, 640:1280]
        hid[c, :, 0:640] = (g * jax.nn.sigmoid(g) * u).astype(BF)
        g = acc[c, :, 1280:1344]
        u = acc[c, :, 1344:1408]
        hid[c, :, 640:704] = (g * jax.nn.sigmoid(g) * u).astype(BF)
    for k in range(8):
        fetch(k, 1).wait()
        part = jnp.zeros((128, 256), F32)
        for c in range(2):
            piece = w[k, :, c, :, 1408:2112].reshape(256, 704)
            part = part + lax.dot_general(hid[c], piece, NT, preferred_element_type=F32)
        out_ref[k] = part.astype(BF)


def on_device(
    sequence_entries,
    former_norm_factor,
    conveyor_matrix,
    conveyor_rescalers,
    blend_value_matrix,
    blend_rescalers,
    blend_norm_factor,
    location_matrices,
    location_offsets,
    branch_emission_matrix,
    emission_rescalers,
    latter_norm_factor,
    valve_matrix,
    valve_rescalers,
    raising_matrix,
    raising_rescalers,
    lowering_matrix,
    lowering_rescalers,
):
    z, x, c = lax.axis_index("z"), lax.axis_index("x"), lax.axis_index("c")
    swap = [(0, 1), (1, 0)]
    own, ffn_own, seqs = pl.pallas_call(
        pack_kernel,
        in_specs=[VM] * 11,
        out_specs=[VM] * 3,
        out_shape=[
            jax.ShapeDtypeStruct((8, 32, 640), BF),
            jax.ShapeDtypeStruct((32, 2112), BF),
            jax.ShapeDtypeStruct((8, 256, 256), BF),
        ],
        name="pack",
    )(
        conveyor_matrix,
        blend_value_matrix,
        branch_emission_matrix.T,
        emission_rescalers,
        valve_matrix,
        valve_rescalers,
        raising_matrix,
        raising_rescalers,
        lowering_matrix.T,
        lowering_rescalers,
        sequence_entries,
    )
    ffn_all = lax.all_gather(ffn_own, ("z", "y", "c"), axis=0, tiled=True)

    first = lax.all_to_all(own, "y", 0, 0, tiled=True)
    rows = lax.all_to_all(seqs, TP, 0, 0, tiled=True)
    left = exchange(first[:4].reshape(1, 128, 640), 0)
    right = exchange(first[4:].reshape(1, 128, 640), 1)
    pieces = left + right
    order = blocks(z)

    gain = former_norm_factor.reshape(8, 1, 256)
    prior, factor = pl.pallas_call(
        early_kernel,
        in_specs=[SM] + [VM] * 10,
        out_specs=[VM, VM],
        out_shape=[jax.ShapeDtypeStruct((256, 384), F32), jax.ShapeDtypeStruct((256, 128), F32)],
        name="early",
    )(order, rows, gain, *left[:4], *right[:4])
    act, own_sq = pl.pallas_call(
        project_kernel,
        in_specs=[SM] + [VM] * 8,
        out_specs=[VM, VM],
        out_shape=[jax.ShapeDtypeStruct((256, 384), F32), jax.ShapeDtypeStruct((1, 1, 256), F32)],
        name="project",
    )(order, rows, gain, conveyor_rescalers, blend_rescalers, prior, factor, left[4], right[4])
    all_sq = lax.all_gather(own_sq, TP, axis=0, tiled=True)
    kept, sent = pl.pallas_call(
        gate_kernel,
        in_specs=[SM, SM] + [VM] * 15,
        out_specs=[VM, VM],
        out_shape=[jax.ShapeDtypeStruct((8, 128, 256), BF)] * 2,
        scratch_shapes=[pltpu.VMEM((2, 128, 192), BF)],
        name="gating",
    )(
        order,
        c.astype(jnp.int32).reshape(1),
        act,
        all_sq,
        location_matrices,
        location_offsets,
        blend_norm_factor,
        *pieces,
    )
    got = lax.ppermute(sent, "c", swap)
    both = (kept.astype(F32) + got.astype(F32)).astype(BF).reshape(4, 2, 128, 256)
    shares = lax.all_to_all(both, "x", 0, 0, tiled=True)
    base = lax.dynamic_slice(rows, (2 * x, 128 * c, 0), (2, 128, 256))
    mid_own = (base.astype(F32) + jnp.sum(shares.astype(F32), axis=0)).astype(BF)
    mid = from_everyone(mid_own, "x").reshape(8, 128, 256)
    outs = pl.pallas_call(
        ffn_kernel,
        in_specs=[VM, VM, ANY],
        out_specs=VM,
        out_shape=jax.ShapeDtypeStruct((8, 128, 256), BF),
        scratch_shapes=[
            pltpu.VMEM((8, 8, 2, 32, 2112), BF),
            pltpu.VMEM((2, 128, 1408), F32),
            pltpu.VMEM((2, 128, 704), BF),
            pltpu.SemaphoreType.DMA((2, 8)),
        ],
        name="ffn",
    )(mid, latter_norm_factor.reshape(8, 1, 256), ffn_all.reshape(8, 8, 2, 32, 2112))
    ffn_shares = lax.all_to_all(outs, TP, 0, 0, tiled=True).reshape(4, 2, 128, 256)
    mid_kept = lax.dynamic_index_in_dim(mid_own, c, 0, keepdims=False)
    mid_sent = lax.dynamic_index_in_dim(mid_own, 1 - c, 0, keepdims=False)
    mid_got = lax.ppermute(mid_sent, "c", swap)
    lower = jnp.where(c == 0, mid_kept, mid_got)
    upper = jnp.where(c == 0, mid_got, mid_kept)
    mid_here = jnp.stack([lower, upper])
    out = mid_here.astype(F32) + jnp.sum(ffn_shares.astype(F32), axis=0)
    return out.astype(BF).reshape(256, 256)


def solution(mesh):
    finer = Mesh(mesh.devices.reshape(8, 8, 4, 2), ("z", "y", "x", "c"))
    return jax.shard_map(
        on_device,
        mesh=finer,
        in_specs=(
            P(FS, TP),
            P(),
            P(FS, TP),
            P(TP),
            P(FS, TP),
            P(TP),
            P(TP),
            P(TP, None, None),
            P(TP, None),
            P(TP, FS),
            P(FS),
            P(),
            P(FS, TP),
            P(TP),
            P(FS, TP),
            P(TP),
            P(TP, FS),
            P(FS),
        ),
        out_specs=P(FS, TP),
        check_vma=False,
    )
```

```python
import jax
import jax.numpy as jnp
from jax import lax
from jax.experimental import pallas as pl
from jax.experimental.pallas import tpu as pltpu
from jax.sharding import Mesh
from jax.sharding import PartitionSpec as P

FS = ("z", "y")
TP = ("x", "c")
EPS = 1e-06
BF = jnp.bfloat16
F32 = jnp.float32
NT = (((1,), (1,)), ((), ()))
VM = pl.BlockSpec(memory_space=pltpu.VMEM)
SM = pl.BlockSpec(memory_space=pltpu.SMEM)
ANY = pl.BlockSpec(memory_space=pl.ANY)


def from_everyone(x, axis):
    copies = jnp.broadcast_to(x, (lax.axis_size(axis), *x.shape))
    return lax.all_to_all(copies, axis, split_axis=0, concat_axis=0, tiled=True)


def gelu(v):
    return 0.5 * v * (1.0 + jnp.tanh(0.7978845608028654 * (v + 0.044715 * v * v * v)))


def upright(row, n):
    same = lax.broadcasted_iota(jnp.int32, (n, n), 0) == lax.broadcasted_iota(jnp.int32, (n, n), 1)
    return jnp.sum(jnp.where(same, row.reshape(1, n), 0.0), axis=1, keepdims=True)


def pack_kernel(conv, blend, emis, emis_s, valve, valve_s, raising, raising_s, low, low_s, seq, *refs):
    own, ffn, seqs, scales = refs[7:11]
    scales[:, 0:192] = refs[0][...].reshape(1, 192)
    scales[:, 192:384] = refs[1][...].reshape(1, 192)
    for here, there in zip(refs[2:7], refs[11:]):
        there[...] = here[...]
    emission = emis[...] * upright(emis_s[...], 32)
    packed = jnp.concatenate([conv[...], blend[...], emission, jnp.zeros((32, 64), F32)], axis=1)
    packed = packed.astype(BF)
    for k in range(8):
        own[k] = packed
        seqs[k] = seq[...]
    gate = valve[...] * valve_s[...].reshape(1, 704)
    up = raising[...] * raising_s[...].reshape(1, 704)
    ffn[:, 0:640] = gate[:, 0:640].astype(BF)
    ffn[:, 640:1280] = up[:, 0:640].astype(BF)
    ffn[:, 1280:1408] = jnp.concatenate([gate[:, 640:704], up[:, 640:704]], axis=1).astype(BF)
    ffn[:, 1408:2112] = (low[...] * upright(low_s[...], 32)).astype(BF)


def spread(order, left, right, place=0):
    found = []
    for half, refs in enumerate((left, right)):
        at = place
        for ref in refs:
            for k in range(ref.shape[0]):
                found.append((order[half, at], half, ref, k))
                at += 1
    return found


def multiply(found, x_ref, gain, factor, prior):
    for block, half, ref, k in found:
        cols = pl.ds(128 * half, 128)
        rows = (x_ref[block, :, cols].astype(F32) * factor * gain[block, :, cols]).astype(BF)
        prior = prior + jnp.dot(rows, ref[k, :, 0:384], preferred_element_type=F32)
    return prior


def early_kernel(order, x_ref, gain, *refs):
    pieces, prior_ref, factor_ref = refs[:8], refs[8], refs[9]
    total = jnp.zeros((256, 1), F32)
    for k in range(8):
        v = x_ref[k].astype(F32)
        total = total + jnp.sum(v * v, axis=1, keepdims=True)
    factor = lax.rsqrt(total / 2048.0 + EPS)
    factor_ref[...] = jnp.broadcast_to(factor, (256, 128))
    found = spread(order, pieces[:4], pieces[4:])
    prior_ref[...] = multiply(found, x_ref, gain, factor, jnp.zeros((256, 384), F32))


def project_kernel(order, x_ref, gain, scales, prior, factor, left, right, act_ref, sq_ref):
    found = spread(order, [left], [right], 6)
    prior = multiply(found, x_ref, gain, factor[:, 0:1], prior[...])
    act = gelu(prior * scales[...])
    act_ref[...] = act
    signal = act[:, 192:384]
    ones = jnp.ones((8, 192), F32)
    sums = lax.dot_general(
        ones, signal * signal, NT, precision=lax.Precision.HIGHEST, preferred_element_type=F32
    )
    sq_ref[0] = sums[0:1]


def gate_kernel(order, core, act_ref, sq_ref, mats, offs, gain, *refs):
    pieces, kept, sent, gated = refs[:10], refs[10], refs[11], refs[12]
    total = jnp.sum(sq_ref[...], axis=0)
    factor = lax.rsqrt(total / 1536.0 + EPS)
    rows = lax.broadcasted_iota(jnp.int32, (128, 128), 0)
    cols = lax.broadcasted_iota(jnp.int32, (128, 128), 1)
    lower = cols <= rows
    gains = gain[...]
    for g in range(3):
        mat = jnp.where(lower, mats[g].astype(F32), 0.0)
        for b in range(2):
            at = pl.ds(128 * b, 128)
            mix = (mat * factor[:, 128 * b : 128 * b + 128]).astype(BF)
            sig = (act_ref[at, 192 + 64 * g : 256 + 64 * g] * gains[:, 64 * g : 64 * g + 64]).astype(BF)
            mixed = jnp.dot(mix, sig, preferred_element_type=F32) + upright(offs[g], 128)
            gated[b, :, 64 * g : 64 * g + 64] = (
                act_ref[at, 64 * g : 64 * g + 64] * mixed
            ).astype(BF)
    here = core[0]
    mine, other = gated[here], gated[1 - here]
    for block, half, ref, k in spread(order, pieces[:5], pieces[5:]):
        piece = ref[k, :, 384:576]
        cols = pl.ds(128 * half, 128)
        part = lax.dot_general(mine, piece, NT, preferred_element_type=F32)
        kept[block, :, cols] = part.astype(BF)
        part = lax.dot_general(other, piece, NT, preferred_element_type=F32)
        sent[block, :, cols] = part.astype(BF)


def exchange(own, flip):
    to_pair = [(i, (((i + flip) ^ 1) - flip) % 8) for i in range(8)]
    to_next = [(i, (((i + 1 - flip) ^ 1) - 1 + flip) % 8) for i in range(8)]
    got = lax.ppermute(own, "z", to_pair)
    batch = jnp.concatenate([own, got])
    pieces = [own, got]
    for turn in (to_next, to_pair, to_next):
        batch = lax.ppermute(batch, "z", turn)
        pieces.append(batch)
    return pieces


def blocks(z):
    out = 2 * ((z + jnp.arange(2)) & 1) - 1
    steps = jnp.array([0, -1, 1, 2, -2, -3, 3, 4])
    return ((z + out[:, None] * steps) & 7).astype(jnp.int32)


def ffn_kernel(mid_ref, gain, w_ref, out_ref, w, acc, hid, sems):
    def fetch(n):
        part, k = divmod(n, 8)
        cols = pl.ds(1408 * part, 1408 - 704 * part)
        at = (k, slice(None), slice(None), slice(None), cols)
        return pltpu.make_async_copy(w_ref.at[at], w.at[at], sems.at[n])

    for n in range(3):
        fetch(n).start()

    def arrive(n):
        fetch(n).wait()
        if n + 3 < 16:
            fetch(n + 3).start()

    total = jnp.zeros((128, 1), F32)
    for k in range(8):
        v = mid_ref[k].astype(F32)
        total = total + jnp.sum(v * v, axis=1, keepdims=True)
    factor = lax.rsqrt(total / 2048.0 + EPS)
    for k in range(8):
        rows = (mid_ref[k].astype(F32) * factor * gain[k]).astype(BF)
        arrive(k)
        for c in range(2):
            piece = w[k, :, c, :, 0:1408].reshape(256, 1408)
            part = jnp.dot(rows, piece, preferred_element_type=F32)
            if k == 0:
                acc[c] = part
            else:
                acc[c] = acc[c] + part
    for c in range(2):
        g = acc[c, :, 0:640]
        u = acc[c, :, 640:1280]
        hid[c, :, 0:640] = (g * jax.nn.sigmoid(g) * u).astype(BF)
        g = acc[c, :, 1280:1344]
        u = acc[c, :, 1344:1408]
        hid[c, :, 640:704] = (g * jax.nn.sigmoid(g) * u).astype(BF)
    for k in range(8):
        arrive(8 + k)
        part = jnp.zeros((128, 256), F32)
        for c in range(2):
            piece = w[k, :, c, :, 1408:2112].reshape(256, 704)
            part = part + lax.dot_general(hid[c], piece, NT, preferred_element_type=F32)
        out_ref[k] = part.astype(BF)


def on_device(
    sequence_entries,
    former_norm_factor,
    conveyor_matrix,
    conveyor_rescalers,
    blend_value_matrix,
    blend_rescalers,
    blend_norm_factor,
    location_matrices,
    location_offsets,
    branch_emission_matrix,
    emission_rescalers,
    latter_norm_factor,
    valve_matrix,
    valve_rescalers,
    raising_matrix,
    raising_rescalers,
    lowering_matrix,
    lowering_rescalers,
):
    z, x, c = lax.axis_index("z"), lax.axis_index("x"), lax.axis_index("c")
    swap = [(0, 1), (1, 0)]
    own, ffn_own, seqs, scales, gain, latter_gain, mats, offs, blend_gain = pl.pallas_call(
        pack_kernel,
        in_specs=[VM] * 18,
        out_specs=[VM] * 9,
        out_shape=[
            jax.ShapeDtypeStruct((8, 32, 640), BF),
            jax.ShapeDtypeStruct((32, 2112), BF),
            jax.ShapeDtypeStruct((8, 256, 256), BF),
            pltpu.VMEM((1, 384), F32),
            pltpu.VMEM((8, 1, 256), F32),
            pltpu.VMEM((8, 1, 256), F32),
            pltpu.VMEM((3, 128, 128), BF),
            pltpu.VMEM((3, 128), F32),
            pltpu.VMEM((1, 192), F32),
        ],
        name="pack",
    )(
        conveyor_matrix,
        blend_value_matrix,
        branch_emission_matrix.T,
        emission_rescalers,
        valve_matrix,
        valve_rescalers,
        raising_matrix,
        raising_rescalers,
        lowering_matrix.T,
        lowering_rescalers,
        sequence_entries,
        conveyor_rescalers,
        blend_rescalers,
        former_norm_factor.reshape(8, 1, 256),
        latter_norm_factor.reshape(8, 1, 256),
        location_matrices,
        location_offsets,
        blend_norm_factor.reshape(1, 192),
    )
    ffn_all = lax.all_gather(ffn_own, ("z", "y", "c"), axis=0, tiled=True)

    first = lax.all_to_all(own, "y", 0, 0, tiled=True)
    rows = lax.all_to_all(seqs, TP, 0, 0, tiled=True)
    left = [vmem(p) for p in exchange(first[:4].reshape(1, 128, 640), 0)]
    right = [vmem(p) for p in exchange(first[4:].reshape(1, 128, 640), 1)]
    pieces = left + right
    order = blocks(z)
    near = vmem(rows)

    prior, factor = pl.pallas_call(
        early_kernel,
        in_specs=[SM] + [VM] * 10,
        out_specs=[VM, VM],
        out_shape=[pltpu.VMEM((256, 384), F32), pltpu.VMEM((256, 128), F32)],
        compiler_params=limit(4),
        name="early",
    )(order, near, gain, *left[:4], *right[:4])
    act, own_sq = pl.pallas_call(
        project_kernel,
        in_specs=[SM] + [VM] * 7,
        out_specs=[VM, VM],
        out_shape=[pltpu.VMEM((256, 384), F32), jax.ShapeDtypeStruct((1, 1, 256), F32)],
        compiler_params=limit(4),
        name="project",
    )(order, near, gain, scales, prior, factor, left[4], right[4])
    all_sq = lax.all_gather(own_sq, TP, axis=0, tiled=True)
    kept, sent = pl.pallas_call(
        gate_kernel,
        in_specs=[SM, SM] + [VM] * 15,
        out_specs=[VM, VM],
        out_shape=[jax.ShapeDtypeStruct((8, 128, 256), BF)] * 2,
        scratch_shapes=[pltpu.VMEM((2, 128, 192), BF)],
        compiler_params=limit(6),
        name="gating",
    )(
        order,
        c.astype(jnp.int32).reshape(1),
        act,
        all_sq,
        mats,
        offs,
        blend_gain,
        *pieces,
    )
    got = lax.ppermute(sent, "c", swap)
    both = (kept.astype(F32) + got.astype(F32)).astype(BF).reshape(4, 2, 128, 256)
    shares = lax.all_to_all(both, "x", 0, 0, tiled=True)
    base = lax.dynamic_slice(rows, (2 * x, 128 * c, 0), (2, 128, 256))
    mid_own = (base.astype(F32) + jnp.sum(shares.astype(F32), axis=0)).astype(BF)
    mid = from_everyone(mid_own, "x").reshape(8, 128, 256)
    outs = pl.pallas_call(
        ffn_kernel,
        in_specs=[VM, VM, pl.BlockSpec(memory_space=pltpu.HBM)],
        out_specs=VM,
        out_shape=jax.ShapeDtypeStruct((8, 128, 256), BF),
        scratch_shapes=[
            pltpu.VMEM((8, 8, 2, 32, 2112), BF),
            pltpu.VMEM((2, 128, 1408), F32),
            pltpu.VMEM((2, 128, 704), BF),
            pltpu.SemaphoreType.DMA((16,)),
        ],
        name="ffn",
    )(vmem(mid), latter_gain, ffn_all.reshape(8, 8, 2, 32, 2112))
    ffn_shares = lax.all_to_all(outs, TP, 0, 0, tiled=True).reshape(4, 2, 128, 256)
    mid_kept = lax.dynamic_index_in_dim(mid_own, c, 0, keepdims=False)
    mid_sent = lax.dynamic_index_in_dim(mid_own, 1 - c, 0, keepdims=False)
    mid_got = lax.ppermute(mid_sent, "c", swap)
    lower = jnp.where(c == 0, mid_kept, mid_got)
    upper = jnp.where(c == 0, mid_got, mid_kept)
    mid_here = jnp.stack([lower, upper])
    out = mid_here.astype(F32) + jnp.sum(ffn_shares.astype(F32), axis=0)
    return out.astype(BF).reshape(256, 256)


def limit(mib):
    return pltpu.CompilerParams(vmem_limit_bytes=mib << 20)


def vmem(x):
    return pltpu.with_memory_space_constraint(x, pltpu.VMEM)


def solution(mesh):
    finer = Mesh(mesh.devices.reshape(8, 8, 4, 2), ("z", "y", "x", "c"))
    return jax.shard_map(
        on_device,
        mesh=finer,
        in_specs=(
            P(FS, TP),
            P(),
            P(FS, TP),
            P(TP),
            P(FS, TP),
            P(TP),
            P(TP),
            P(TP, None, None),
            P(TP, None),
            P(TP, FS),
            P(FS),
            P(),
            P(FS, TP),
            P(TP),
            P(FS, TP),
            P(TP),
            P(TP, FS),
            P(FS),
        ),
        out_specs=P(FS, TP),
        check_vma=False,
    )
```

```python
import jax
import jax.numpy as jnp
from jax import lax
from jax.experimental import pallas as pl
from jax.experimental.pallas import tpu as pltpu
from jax.sharding import Mesh
from jax.sharding import PartitionSpec as P

FS = ("z", "y")
TP = ("x", "c")
EPS = 1e-06
BF = jnp.bfloat16
F32 = jnp.float32
NT = (((1,), (1,)), ((), ()))
VM = pl.BlockSpec(memory_space=pltpu.VMEM)
SM = pl.BlockSpec(memory_space=pltpu.SMEM)
ANY = pl.BlockSpec(memory_space=pl.ANY)


def from_everyone(x, axis):
    copies = jnp.broadcast_to(x, (lax.axis_size(axis), *x.shape))
    return lax.all_to_all(copies, axis, split_axis=0, concat_axis=0, tiled=True)


def gelu(v):
    return 0.5 * v * (1.0 + jnp.tanh(0.7978845608028654 * (v + 0.044715 * v * v * v)))


def upright(row, n):
    same = lax.broadcasted_iota(jnp.int32, (n, n), 0) == lax.broadcasted_iota(jnp.int32, (n, n), 1)
    return jnp.sum(jnp.where(same, row.reshape(1, n), 0.0), axis=1, keepdims=True)


def pack_kernel(conv, blend, emis, emis_s, valve, valve_s, raising, raising_s, low, low_s, seq, *refs):
    own, ffn, seqs, scales = refs[7:11]
    scales[:, 0:192] = refs[0][...].reshape(1, 192)
    scales[:, 192:384] = refs[1][...].reshape(1, 192)
    for here, there in zip(refs[2:7], refs[11:]):
        there[...] = here[...]
    emission = emis[...] * upright(emis_s[...], 32)
    packed = jnp.concatenate([conv[...], blend[...], emission, jnp.zeros((32, 64), F32)], axis=1)
    packed = packed.astype(BF)
    for k in range(8):
        own[k] = packed
        seqs[k] = seq[...]
    gate = valve[...] * valve_s[...].reshape(1, 704)
    up = raising[...] * raising_s[...].reshape(1, 704)
    ffn[:, 0:640] = gate[:, 0:640].astype(BF)
    ffn[:, 640:1280] = up[:, 0:640].astype(BF)
    ffn[:, 1280:1408] = jnp.concatenate([gate[:, 640:704], up[:, 640:704]], axis=1).astype(BF)
    ffn[:, 1408:2112] = (low[...] * upright(low_s[...], 32)).astype(BF)


def spread(order, left, right, place=0):
    found = []
    for half, refs in enumerate((left, right)):
        at = place
        for ref in refs:
            for k in range(ref.shape[0]):
                found.append((order[half, at], half, ref, k))
                at += 1
    return found


def multiply(found, x_ref, gain, factor, prior):
    for block, half, ref, k in found:
        cols = pl.ds(128 * half, 128)
        rows = (x_ref[block, :, cols].astype(F32) * factor * gain[block, :, cols]).astype(BF)
        prior = prior + jnp.dot(rows, ref[k, :, 0:384], preferred_element_type=F32)
    return prior


def early_kernel(order, x_ref, gain, *refs):
    pieces, prior_ref, factor_ref = refs[:6], refs[6], refs[7]
    total = jnp.zeros((256, 1), F32)
    for k in range(8):
        v = x_ref[k].astype(F32)
        total = total + jnp.sum(v * v, axis=1, keepdims=True)
    factor = lax.rsqrt(total / 2048.0 + EPS)
    factor_ref[...] = jnp.broadcast_to(factor, (256, 128))
    found = spread(order, pieces[:3], pieces[3:])
    prior_ref[...] = multiply(found, x_ref, gain, factor, jnp.zeros((256, 384), F32))


def project_kernel(order, x_ref, gain, scales, prior, factor, left, right, act_ref, sq_ref):
    found = spread(order, [left], [right], 6)
    prior = multiply(found, x_ref, gain, factor[:, 0:1], prior[...])
    act = gelu(prior * scales[...])
    act_ref[...] = act
    signal = act[:, 192:384]
    ones = jnp.ones((8, 192), F32)
    sums = lax.dot_general(
        ones, signal * signal, NT, precision=lax.Precision.HIGHEST, preferred_element_type=F32
    )
    sq_ref[0] = sums[0:1]


def gate_kernel(order, core, act_ref, sq_ref, mats, offs, gain, *refs):
    pieces, kept, sent, gated = refs[:8], refs[8], refs[9], refs[10]
    total = jnp.sum(sq_ref[...], axis=0)
    factor = lax.rsqrt(total / 1536.0 + EPS)
    rows = lax.broadcasted_iota(jnp.int32, (128, 128), 0)
    cols = lax.broadcasted_iota(jnp.int32, (128, 128), 1)
    lower = cols <= rows
    gains = gain[...]
    for g in range(3):
        mat = jnp.where(lower, mats[g].astype(F32), 0.0)
        for b in range(2):
            at = pl.ds(128 * b, 128)
            mix = (mat * factor[:, 128 * b : 128 * b + 128]).astype(BF)
            sig = (act_ref[at, 192 + 64 * g : 256 + 64 * g] * gains[:, 64 * g : 64 * g + 64]).astype(BF)
            mixed = jnp.dot(mix, sig, preferred_element_type=F32) + upright(offs[g], 128)
            gated[b, :, 64 * g : 64 * g + 64] = (
                act_ref[at, 64 * g : 64 * g + 64] * mixed
            ).astype(BF)
    here = core[0]
    mine, other = gated[here], gated[1 - here]
    for block, half, ref, k in spread(order, pieces[:4], pieces[4:]):
        piece = ref[k, :, 0:192]
        cols = pl.ds(128 * half, 128)
        part = lax.dot_general(mine, piece, NT, preferred_element_type=F32)
        kept[block, :, cols] = part.astype(BF)
        part = lax.dot_general(other, piece, NT, preferred_element_type=F32)
        sent[block, :, cols] = part.astype(BF)


def exchange(own, flip):
    to_pair = [(i, (((i + flip) ^ 1) - flip) % 8) for i in range(8)]
    to_next = [(i, (((i + 1 - flip) ^ 1) - 1 + flip) % 8) for i in range(8)]
    got = lax.ppermute(own, "z", to_pair)
    batch = jnp.concatenate([own, got])
    pieces = [batch]
    for turn in (to_next, to_pair, to_next):
        batch = lax.ppermute(batch, "z", turn)
        pieces.append(batch)
    return pieces


def blocks(z):
    out = 2 * ((z + jnp.arange(2)) & 1) - 1
    steps = jnp.array([0, -1, 1, 2, -2, -3, 3, 4])
    return ((z + out[:, None] * steps) & 7).astype(jnp.int32)


def ffn_kernel(mid_ref, gain, w_ref, out_ref, w, acc, hid, sems):
    def fetch(n):
        part, k = divmod(n, 8)
        cols = pl.ds(1408 * part, 1408 - 704 * part)
        at = (k, slice(None), slice(None), slice(None), cols)
        return pltpu.make_async_copy(w_ref.at[at], w.at[at], sems.at[n])

    for n in range(3):
        fetch(n).start()

    def arrive(n):
        fetch(n).wait()
        if n + 3 < 16:
            fetch(n + 3).start()

    total = jnp.zeros((128, 1), F32)
    for k in range(8):
        v = mid_ref[k].astype(F32)
        total = total + jnp.sum(v * v, axis=1, keepdims=True)
    factor = lax.rsqrt(total / 2048.0 + EPS)
    for k in range(8):
        rows = (mid_ref[k].astype(F32) * factor * gain[k]).astype(BF)
        arrive(k)
        for c in range(2):
            piece = w[k, :, c, :, 0:1408].reshape(256, 1408)
            part = jnp.dot(rows, piece, preferred_element_type=F32)
            if k == 0:
                acc[c] = part
            else:
                acc[c] = acc[c] + part
    for c in range(2):
        g = acc[c, :, 0:640]
        u = acc[c, :, 640:1280]
        hid[c, :, 0:640] = (g * jax.nn.sigmoid(g) * u).astype(BF)
        g = acc[c, :, 1280:1344]
        u = acc[c, :, 1344:1408]
        hid[c, :, 640:704] = (g * jax.nn.sigmoid(g) * u).astype(BF)
    for k in range(8):
        arrive(8 + k)
        part = jnp.zeros((128, 256), F32)
        for c in range(2):
            piece = w[k, :, c, :, 1408:2112].reshape(256, 704)
            part = part + lax.dot_general(hid[c], piece, NT, preferred_element_type=F32)
        out_ref[k] = part.astype(BF)


def on_device(
    sequence_entries,
    former_norm_factor,
    conveyor_matrix,
    conveyor_rescalers,
    blend_value_matrix,
    blend_rescalers,
    blend_norm_factor,
    location_matrices,
    location_offsets,
    branch_emission_matrix,
    emission_rescalers,
    latter_norm_factor,
    valve_matrix,
    valve_rescalers,
    raising_matrix,
    raising_rescalers,
    lowering_matrix,
    lowering_rescalers,
):
    z, x, c = lax.axis_index("z"), lax.axis_index("x"), lax.axis_index("c")
    swap = [(0, 1), (1, 0)]
    own, ffn_own, seqs, scales, gain, latter_gain, mats, offs, blend_gain = pl.pallas_call(
        pack_kernel,
        in_specs=[VM] * 18,
        out_specs=[VM] * 9,
        out_shape=[
            jax.ShapeDtypeStruct((8, 32, 640), BF),
            jax.ShapeDtypeStruct((32, 2112), BF),
            jax.ShapeDtypeStruct((8, 256, 256), BF),
            pltpu.VMEM((1, 384), F32),
            pltpu.VMEM((8, 1, 256), F32),
            pltpu.VMEM((8, 1, 256), F32),
            pltpu.VMEM((3, 128, 128), BF),
            pltpu.VMEM((3, 128), F32),
            pltpu.VMEM((1, 192), F32),
        ],
        name="pack",
    )(
        conveyor_matrix,
        blend_value_matrix,
        branch_emission_matrix.T,
        emission_rescalers,
        valve_matrix,
        valve_rescalers,
        raising_matrix,
        raising_rescalers,
        lowering_matrix.T,
        lowering_rescalers,
        sequence_entries,
        conveyor_rescalers,
        blend_rescalers,
        former_norm_factor.reshape(8, 1, 256),
        latter_norm_factor.reshape(8, 1, 256),
        location_matrices,
        location_offsets,
        blend_norm_factor.reshape(1, 192),
    )
    ffn_all = lax.all_gather(ffn_own, ("z", "y", "c"), axis=0, tiled=True)

    first = lax.all_to_all(own, "y", 0, 0, tiled=True)
    rows = lax.all_to_all(seqs, TP, 0, 0, tiled=True)
    streams = {}
    for name, cols in (("cb", slice(0, 384)), ("em", slice(384, 640))):
        for flip in range(2):
            half = first[4 * flip : 4 * flip + 4, :, cols].reshape(1, 128, -1)
            streams[name, flip] = [vmem(p) for p in exchange(half, flip)]
    left, right = streams["cb", 0], streams["cb", 1]
    pieces = streams["em", 0] + streams["em", 1]
    order = blocks(z)
    near = vmem(rows)

    prior, factor = pl.pallas_call(
        early_kernel,
        in_specs=[SM] + [VM] * 8,
        out_specs=[VM, VM],
        out_shape=[pltpu.VMEM((256, 384), F32), pltpu.VMEM((256, 128), F32)],
        compiler_params=limit(4),
        name="early",
    )(order, near, gain, *left[:3], *right[:3])
    act, own_sq = pl.pallas_call(
        project_kernel,
        in_specs=[SM] + [VM] * 7,
        out_specs=[VM, VM],
        out_shape=[pltpu.VMEM((256, 384), F32), jax.ShapeDtypeStruct((1, 1, 256), F32)],
        compiler_params=limit(4),
        name="project",
    )(order, near, gain, scales, prior, factor, left[3], right[3])
    all_sq = lax.all_gather(own_sq, TP, axis=0, tiled=True)
    kept, sent = pl.pallas_call(
        gate_kernel,
        in_specs=[SM, SM] + [VM] * 13,
        out_specs=[VM, VM],
        out_shape=[jax.ShapeDtypeStruct((8, 128, 256), BF)] * 2,
        scratch_shapes=[pltpu.VMEM((2, 128, 192), BF)],
        compiler_params=limit(6),
        name="gating",
    )(
        order,
        c.astype(jnp.int32).reshape(1),
        act,
        all_sq,
        mats,
        offs,
        blend_gain,
        *pieces,
    )
    got = lax.ppermute(sent, "c", swap)
    both = (kept.astype(F32) + got.astype(F32)).astype(BF).reshape(4, 2, 128, 256)
    shares = lax.all_to_all(both, "x", 0, 0, tiled=True)
    base = lax.dynamic_slice(rows, (2 * x, 128 * c, 0), (2, 128, 256))
    mid_own = (base.astype(F32) + jnp.sum(shares.astype(F32), axis=0)).astype(BF)
    mid = from_everyone(mid_own, "x").reshape(8, 128, 256)
    outs = pl.pallas_call(
        ffn_kernel,
        in_specs=[VM, VM, pl.BlockSpec(memory_space=pltpu.HBM)],
        out_specs=VM,
        out_shape=jax.ShapeDtypeStruct((8, 128, 256), BF),
        scratch_shapes=[
            pltpu.VMEM((8, 8, 2, 32, 2112), BF),
            pltpu.VMEM((2, 128, 1408), F32),
            pltpu.VMEM((2, 128, 704), BF),
            pltpu.SemaphoreType.DMA((16,)),
        ],
        name="ffn",
    )(vmem(mid), latter_gain, ffn_all.reshape(8, 8, 2, 32, 2112))
    ffn_shares = lax.all_to_all(outs, TP, 0, 0, tiled=True).reshape(4, 2, 128, 256)
    mid_kept = lax.dynamic_index_in_dim(mid_own, c, 0, keepdims=False)
    mid_sent = lax.dynamic_index_in_dim(mid_own, 1 - c, 0, keepdims=False)
    mid_got = lax.ppermute(mid_sent, "c", swap)
    lower = jnp.where(c == 0, mid_kept, mid_got)
    upper = jnp.where(c == 0, mid_got, mid_kept)
    mid_here = jnp.stack([lower, upper])
    out = mid_here.astype(F32) + jnp.sum(ffn_shares.astype(F32), axis=0)
    return out.astype(BF).reshape(256, 256)


def limit(mib):
    return pltpu.CompilerParams(vmem_limit_bytes=mib << 20)


def vmem(x):
    return pltpu.with_memory_space_constraint(x, pltpu.VMEM)


def solution(mesh):
    finer = Mesh(mesh.devices.reshape(8, 8, 4, 2), ("z", "y", "x", "c"))
    return jax.shard_map(
        on_device,
        mesh=finer,
        in_specs=(
            P(FS, TP),
            P(),
            P(FS, TP),
            P(TP),
            P(FS, TP),
            P(TP),
            P(TP),
            P(TP, None, None),
            P(TP, None),
            P(TP, FS),
            P(FS),
            P(),
            P(FS, TP),
            P(TP),
            P(FS, TP),
            P(TP),
            P(TP, FS),
            P(FS),
        ),
        out_specs=P(FS, TP),
        check_vma=False,
    )
```

```python
import jax
import jax.numpy as jnp
from jax import lax
from jax.experimental import pallas as pl
from jax.experimental.pallas import tpu as pltpu
from jax.sharding import Mesh
from jax.sharding import PartitionSpec as P

FS = ("z", "y")
TP = ("x", "c")
EPS = 1e-06
BF = jnp.bfloat16
F32 = jnp.float32
NT = (((1,), (1,)), ((), ()))
VM = pl.BlockSpec(memory_space=pltpu.VMEM)
SM = pl.BlockSpec(memory_space=pltpu.SMEM)
ANY = pl.BlockSpec(memory_space=pl.ANY)


def from_everyone(x, axis):
    copies = jnp.broadcast_to(x, (lax.axis_size(axis), *x.shape))
    return lax.all_to_all(copies, axis, split_axis=0, concat_axis=0, tiled=True)


def gelu(v):
    return 0.5 * v * (1.0 + jnp.tanh(0.7978845608028654 * (v + 0.044715 * v * v * v)))


def upright(row, n):
    same = lax.broadcasted_iota(jnp.int32, (n, n), 0) == lax.broadcasted_iota(jnp.int32, (n, n), 1)
    return jnp.sum(jnp.where(same, row.reshape(1, n), 0.0), axis=1, keepdims=True)


def pack_kernel(conv, blend, emis, emis_s, own):
    emission = emis[...] * upright(emis_s[...], 32)
    packed = jnp.concatenate([conv[...], blend[...], emission, jnp.zeros((32, 64), F32)], axis=1)
    packed = packed.astype(BF)
    for k in range(8):
        own[k] = packed


def pack_later_kernel(valve, valve_s, raising, raising_s, low, low_s, seq, *refs):
    ffn, seqs, scales = refs[7:10]
    scales[:, 0:192] = refs[0][...].reshape(1, 192)
    scales[:, 192:384] = refs[1][...].reshape(1, 192)
    for here, there in zip(refs[2:7], refs[10:]):
        there[...] = here[...]
    for k in range(8):
        seqs[k] = seq[...]
    gate = valve[...] * valve_s[...].reshape(1, 704)
    up = raising[...] * raising_s[...].reshape(1, 704)
    ffn[:, 0:640] = gate[:, 0:640].astype(BF)
    ffn[:, 640:1280] = up[:, 0:640].astype(BF)
    ffn[:, 1280:1408] = jnp.concatenate([gate[:, 640:704], up[:, 640:704]], axis=1).astype(BF)
    ffn[:, 1408:2112] = (low[...] * upright(low_s[...], 32)).astype(BF)


def spread(order, left, right, place=0):
    found = []
    for half, refs in enumerate((left, right)):
        at = place
        for ref in refs:
            for k in range(ref.shape[0]):
                found.append((order[half, at], half, ref, k))
                at += 1
    return found


def multiply(found, x_ref, gain, factor, prior):
    for block, half, ref, k in found:
        cols = pl.ds(128 * half, 128)
        rows = (x_ref[block, :, cols].astype(F32) * factor * gain[block, :, cols]).astype(BF)
        prior = prior + jnp.dot(rows, ref[k, :, 0:384], preferred_element_type=F32)
    return prior


def early_kernel(order, x_ref, gain, *refs):
    pieces, prior_ref, factor_ref = refs[:6], refs[6], refs[7]
    total = jnp.zeros((256, 1), F32)
    for k in range(8):
        v = x_ref[k].astype(F32)
        total = total + jnp.sum(v * v, axis=1, keepdims=True)
    factor = lax.rsqrt(total / 2048.0 + EPS)
    factor_ref[...] = jnp.broadcast_to(factor, (256, 128))
    found = spread(order, pieces[:3], pieces[3:])
    prior_ref[...] = multiply(found, x_ref, gain, factor, jnp.zeros((256, 384), F32))


def project_kernel(order, x_ref, gain, scales, prior, factor, left, right, act_ref, sq_ref):
    found = spread(order, [left], [right], 6)
    prior = multiply(found, x_ref, gain, factor[:, 0:1], prior[...])
    act = gelu(prior * scales[...])
    act_ref[...] = act
    signal = act[:, 192:384]
    ones = jnp.ones((8, 192), F32)
    sums = lax.dot_general(
        ones, signal * signal, NT, precision=lax.Precision.HIGHEST, preferred_element_type=F32
    )
    sq_ref[0] = sums[0:1]


def gate_kernel(order, core, act_ref, sq_ref, mats, offs, gain, *refs):
    pieces, kept, sent, gated = refs[:8], refs[8], refs[9], refs[10]
    total = jnp.sum(sq_ref[...], axis=0)
    factor = lax.rsqrt(total / 1536.0 + EPS)
    rows = lax.broadcasted_iota(jnp.int32, (128, 128), 0)
    cols = lax.broadcasted_iota(jnp.int32, (128, 128), 1)
    lower = cols <= rows
    gains = gain[...]
    for g in range(3):
        mat = jnp.where(lower, mats[g].astype(F32), 0.0)
        for b in range(2):
            at = pl.ds(128 * b, 128)
            mix = (mat * factor[:, 128 * b : 128 * b + 128]).astype(BF)
            sig = (act_ref[at, 192 + 64 * g : 256 + 64 * g] * gains[:, 64 * g : 64 * g + 64]).astype(BF)
            mixed = jnp.dot(mix, sig, preferred_element_type=F32) + upright(offs[g], 128)
            gated[b, :, 64 * g : 64 * g + 64] = (
                act_ref[at, 64 * g : 64 * g + 64] * mixed
            ).astype(BF)
    here = core[0]
    mine, other = gated[here], gated[1 - here]
    for block, half, ref, k in spread(order, pieces[:4], pieces[4:]):
        piece = ref[k, :, 384:576]
        cols = pl.ds(128 * half, 128)
        part = lax.dot_general(mine, piece, NT, preferred_element_type=F32)
        kept[block, :, cols] = part.astype(BF)
        part = lax.dot_general(other, piece, NT, preferred_element_type=F32)
        sent[block, :, cols] = part.astype(BF)


def exchange(own, flip):
    to_pair = [(i, (((i + flip) ^ 1) - flip) % 8) for i in range(8)]
    to_next = [(i, (((i + 1 - flip) ^ 1) - 1 + flip) % 8) for i in range(8)]
    got = lax.ppermute(own, "z", to_pair)
    batch = jnp.concatenate([own, got])
    pieces = [batch]
    for turn in (to_next, to_pair, to_next):
        batch = lax.ppermute(batch, "z", turn)
        pieces.append(batch)
    return pieces


def blocks(z):
    out = 2 * ((z + jnp.arange(2)) & 1) - 1
    steps = jnp.array([0, -1, 1, 2, -2, -3, 3, 4])
    return ((z + out[:, None] * steps) & 7).astype(jnp.int32)


def ffn_kernel(mid_ref, gain, w_ref, out_ref, w, acc, hid, sems):
    def fetch(n):
        part, k = divmod(n, 8)
        cols = pl.ds(1408 * part, 1408 - 704 * part)
        at = (k, slice(None), slice(None), slice(None), cols)
        return pltpu.make_async_copy(w_ref.at[at], w.at[at], sems.at[n])

    for n in range(8):
        fetch(n).start()

    def arrive(n):
        fetch(n).wait()
        if n < 8:
            fetch(n + 8).start()

    total = jnp.zeros((128, 1), F32)
    for k in range(8):
        v = mid_ref[k].astype(F32)
        total = total + jnp.sum(v * v, axis=1, keepdims=True)
    factor = lax.rsqrt(total / 2048.0 + EPS)
    for k in range(8):
        rows = (mid_ref[k].astype(F32) * factor * gain[k]).astype(BF)
        arrive(k)
        for c in range(2):
            piece = w[k, :, c, :, 0:1408].reshape(256, 1408)
            part = jnp.dot(rows, piece, preferred_element_type=F32)
            if k == 0:
                acc[c] = part
            else:
                acc[c] = acc[c] + part
    for c in range(2):
        g = acc[c, :, 0:640]
        u = acc[c, :, 640:1280]
        hid[c, :, 0:640] = (g * jax.nn.sigmoid(g) * u).astype(BF)
        g = acc[c, :, 1280:1344]
        u = acc[c, :, 1344:1408]
        hid[c, :, 640:704] = (g * jax.nn.sigmoid(g) * u).astype(BF)
    for k in range(8):
        if k % 4 == 0:
            for n in range(8 + k, 12 + k):
                arrive(n)
        part = jnp.zeros((128, 256), F32)
        for c in range(2):
            piece = w[k, :, c, :, 1408:2112].reshape(256, 704)
            part = part + lax.dot_general(hid[c], piece, NT, preferred_element_type=F32)
        out_ref[k] = part.astype(BF)


def on_device(
    sequence_entries,
    former_norm_factor,
    conveyor_matrix,
    conveyor_rescalers,
    blend_value_matrix,
    blend_rescalers,
    blend_norm_factor,
    location_matrices,
    location_offsets,
    branch_emission_matrix,
    emission_rescalers,
    latter_norm_factor,
    valve_matrix,
    valve_rescalers,
    raising_matrix,
    raising_rescalers,
    lowering_matrix,
    lowering_rescalers,
):
    z, x, c = lax.axis_index("z"), lax.axis_index("x"), lax.axis_index("c")
    swap = [(0, 1), (1, 0)]
    own = pl.pallas_call(
        pack_kernel,
        in_specs=[VM] * 4,
        out_specs=VM,
        out_shape=jax.ShapeDtypeStruct((8, 32, 640), BF),
        name="pack",
    )(conveyor_matrix, blend_value_matrix, branch_emission_matrix.T, emission_rescalers)
    ffn_own, seqs, scales, gain, latter_gain, mats, offs, blend_gain = pl.pallas_call(
        pack_later_kernel,
        in_specs=[VM] * 14,
        out_specs=[VM] * 8,
        out_shape=[
            jax.ShapeDtypeStruct((32, 2112), BF),
            jax.ShapeDtypeStruct((8, 256, 256), BF),
            pltpu.VMEM((1, 384), F32),
            pltpu.VMEM((8, 1, 256), F32),
            pltpu.VMEM((8, 1, 256), F32),
            pltpu.VMEM((3, 128, 128), BF),
            pltpu.VMEM((3, 128), F32),
            pltpu.VMEM((1, 192), F32),
        ],
        name="pack_later",
    )(
        valve_matrix,
        valve_rescalers,
        raising_matrix,
        raising_rescalers,
        lowering_matrix.T,
        lowering_rescalers,
        sequence_entries,
        conveyor_rescalers,
        blend_rescalers,
        former_norm_factor.reshape(8, 1, 256),
        latter_norm_factor.reshape(8, 1, 256),
        location_matrices,
        location_offsets,
        blend_norm_factor.reshape(1, 192),
    )
    ffn_all = lax.all_gather(ffn_own, ("z", "y", "c"), axis=0, tiled=True)

    first = lax.all_to_all(own, "y", 0, 0, tiled=True)
    rows = lax.all_to_all(seqs, TP, 0, 0, tiled=True)
    left = [vmem(p) for p in exchange(first[:4].reshape(1, 128, 640), 0)]
    right = [vmem(p) for p in exchange(first[4:].reshape(1, 128, 640), 1)]
    pieces = left + right
    order = blocks(z)
    near = vmem(rows)

    prior, factor = pl.pallas_call(
        early_kernel,
        in_specs=[SM] + [VM] * 8,
        out_specs=[VM, VM],
        out_shape=[pltpu.VMEM((256, 384), F32), pltpu.VMEM((256, 128), F32)],
        compiler_params=limit(4),
        name="early",
    )(order, near, gain, *left[:3], *right[:3])
    act, own_sq = pl.pallas_call(
        project_kernel,
        in_specs=[SM] + [VM] * 7,
        out_specs=[VM, VM],
        out_shape=[pltpu.VMEM((256, 384), F32), jax.ShapeDtypeStruct((1, 1, 256), F32)],
        compiler_params=limit(4),
        name="project",
    )(order, near, gain, scales, prior, factor, left[3], right[3])
    all_sq = lax.all_gather(own_sq, TP, axis=0, tiled=True)
    kept, sent = pl.pallas_call(
        gate_kernel,
        in_specs=[SM, SM] + [VM] * 13,
        out_specs=[VM, VM],
        out_shape=[jax.ShapeDtypeStruct((8, 128, 256), BF)] * 2,
        scratch_shapes=[pltpu.VMEM((2, 128, 192), BF)],
        compiler_params=limit(6),
        name="gating",
    )(
        order,
        c.astype(jnp.int32).reshape(1),
        act,
        all_sq,
        mats,
        offs,
        blend_gain,
        *pieces,
    )
    got = lax.ppermute(sent, "c", swap)
    both = (kept.astype(F32) + got.astype(F32)).astype(BF).reshape(4, 2, 128, 256)
    shares = lax.all_to_all(both, "x", 0, 0, tiled=True)
    base = lax.dynamic_slice(rows, (2 * x, 128 * c, 0), (2, 128, 256))
    mid_own = (base.astype(F32) + jnp.sum(shares.astype(F32), axis=0)).astype(BF)
    mid = from_everyone(mid_own, "x").reshape(8, 128, 256)
    outs = pl.pallas_call(
        ffn_kernel,
        in_specs=[VM, VM, pl.BlockSpec(memory_space=pltpu.HBM)],
        out_specs=VM,
        out_shape=jax.ShapeDtypeStruct((8, 128, 256), BF),
        scratch_shapes=[
            pltpu.VMEM((8, 8, 2, 32, 2112), BF),
            pltpu.VMEM((2, 128, 1408), F32),
            pltpu.VMEM((2, 128, 704), BF),
            pltpu.SemaphoreType.DMA((16,)),
        ],
        name="ffn",
    )(vmem(mid), latter_gain, ffn_all.reshape(8, 8, 2, 32, 2112))
    ffn_shares = lax.all_to_all(outs, TP, 0, 0, tiled=True).reshape(4, 2, 128, 256)
    mid_kept = lax.dynamic_index_in_dim(mid_own, c, 0, keepdims=False)
    mid_sent = lax.dynamic_index_in_dim(mid_own, 1 - c, 0, keepdims=False)
    mid_got = lax.ppermute(mid_sent, "c", swap)
    lower = jnp.where(c == 0, mid_kept, mid_got)
    upper = jnp.where(c == 0, mid_got, mid_kept)
    mid_here = jnp.stack([lower, upper])
    out = mid_here.astype(F32) + jnp.sum(ffn_shares.astype(F32), axis=0)
    return out.astype(BF).reshape(256, 256)


def limit(mib):
    return pltpu.CompilerParams(vmem_limit_bytes=mib << 20)


def vmem(x):
    return pltpu.with_memory_space_constraint(x, pltpu.VMEM)


def solution(mesh):
    finer = Mesh(mesh.devices.reshape(8, 8, 4, 2), ("z", "y", "x", "c"))
    return jax.shard_map(
        on_device,
        mesh=finer,
        in_specs=(
            P(FS, TP),
            P(),
            P(FS, TP),
            P(TP),
            P(FS, TP),
            P(TP),
            P(TP),
            P(TP, None, None),
            P(TP, None),
            P(TP, FS),
            P(FS),
            P(),
            P(FS, TP),
            P(TP),
            P(FS, TP),
            P(TP),
            P(TP, FS),
            P(FS),
        ),
        out_specs=P(FS, TP),
        check_vma=False,
    )
```

```python
import jax
import jax.numpy as jnp
from jax import lax
from jax.experimental import pallas as pl
from jax.experimental.pallas import tpu as pltpu
from jax.sharding import Mesh
from jax.sharding import PartitionSpec as P

FS = ("z", "y")
TP = ("x", "c")
EPS = 1e-06
BF = jnp.bfloat16
F32 = jnp.float32
NT = (((1,), (1,)), ((), ()))
VM = pl.BlockSpec(memory_space=pltpu.VMEM)
SM = pl.BlockSpec(memory_space=pltpu.SMEM)
ANY = pl.BlockSpec(memory_space=pl.ANY)


def from_everyone(x, axis):
    copies = jnp.broadcast_to(x, (lax.axis_size(axis), *x.shape))
    return lax.all_to_all(copies, axis, split_axis=0, concat_axis=0, tiled=True)


def gelu(v):
    return 0.5 * v * (1.0 + jnp.tanh(0.7978845608028654 * (v + 0.044715 * v * v * v)))


def upright(row, n):
    same = lax.broadcasted_iota(jnp.int32, (n, n), 0) == lax.broadcasted_iota(jnp.int32, (n, n), 1)
    return jnp.sum(jnp.where(same, row.reshape(1, n), 0.0), axis=1, keepdims=True)


def pack_kernel(conv, blend, emis, emis_s, own):
    emission = emis[...] * upright(emis_s[...], 32)
    packed = jnp.concatenate([conv[...], blend[...], emission, jnp.zeros((32, 64), F32)], axis=1)
    packed = packed.astype(BF)
    for k in range(8):
        own[k] = packed


def pack_ffn_kernel(valve, valve_s, raising, raising_s, low, low_s, ffn):
    gate = valve[...] * valve_s[...].reshape(1, 704)
    up = raising[...] * raising_s[...].reshape(1, 704)
    ffn[:, 0:640] = gate[:, 0:640].astype(BF)
    ffn[:, 640:1280] = up[:, 0:640].astype(BF)
    ffn[:, 1280:1408] = jnp.concatenate([gate[:, 640:704], up[:, 640:704]], axis=1).astype(BF)
    ffn[:, 1408:2112] = (low[...] * upright(low_s[...], 32)).astype(BF)


def keep_kernel(seq, *refs):
    seqs, scales = refs[7:9]
    for k in range(8):
        seqs[k] = seq[...]
    scales[:, 0:192] = refs[0][...].reshape(1, 192)
    scales[:, 192:384] = refs[1][...].reshape(1, 192)
    for here, there in zip(refs[2:7], refs[9:]):
        there[...] = here[...]


def spread(order, left, right, place=0):
    found = []
    for half, refs in enumerate((left, right)):
        at = place
        for ref in refs:
            for k in range(ref.shape[0]):
                found.append((order[half, at], half, ref, k))
                at += 1
    return found


def multiply(found, x_ref, gain, factor, prior):
    for block, half, ref, k in found:
        cols = pl.ds(128 * half, 128)
        rows = (x_ref[block, :, cols].astype(F32) * factor * gain[block, :, cols]).astype(BF)
        prior = prior + jnp.dot(rows, ref[k, :, 0:384], preferred_element_type=F32)
    return prior


def early_kernel(order, x_ref, gain, *refs):
    pieces, prior_ref, factor_ref = refs[:6], refs[6], refs[7]
    total = jnp.zeros((256, 1), F32)
    for k in range(8):
        v = x_ref[k].astype(F32)
        total = total + jnp.sum(v * v, axis=1, keepdims=True)
    factor = lax.rsqrt(total / 2048.0 + EPS)
    factor_ref[...] = jnp.broadcast_to(factor, (256, 128))
    found = spread(order, pieces[:3], pieces[3:])
    prior_ref[...] = multiply(found, x_ref, gain, factor, jnp.zeros((256, 384), F32))


def project_kernel(order, here, x_ref, gain, scales, prior, factor, left, right, act_ref, sq_ref, base):
    base[...] = x_ref[pl.ds(2 * here[0], 2), pl.ds(pl.multiple_of(128 * here[1], 128), 128), :]
    found = spread(order, [left], [right], 6)
    prior = multiply(found, x_ref, gain, factor[:, 0:1], prior[...])
    act = gelu(prior * scales[...])
    act_ref[...] = act
    signal = act[:, 192:384]
    ones = jnp.ones((8, 192), F32)
    sums = lax.dot_general(
        ones, signal * signal, NT, precision=lax.Precision.HIGHEST, preferred_element_type=F32
    )
    sq_ref[...] = jnp.broadcast_to(sums[0:1].reshape(1, 1, 256), (8, 1, 256))


def gate_kernel(order, place, act_ref, sq_ref, mats, offs, gain, *refs):
    pieces, kept, sent, gated = refs[:8], refs[8], refs[9], refs[10]
    total = jnp.sum(sq_ref[...], axis=0)
    factor = lax.rsqrt(total / 1536.0 + EPS)
    rows = lax.broadcasted_iota(jnp.int32, (128, 128), 0)
    cols = lax.broadcasted_iota(jnp.int32, (128, 128), 1)
    lower = cols <= rows
    gains = gain[...]
    for g in range(3):
        mat = jnp.where(lower, mats[g].astype(F32), 0.0)
        for b in range(2):
            at = pl.ds(128 * b, 128)
            mix = (mat * factor[:, 128 * b : 128 * b + 128]).astype(BF)
            sig = (act_ref[at, 192 + 64 * g : 256 + 64 * g] * gains[:, 64 * g : 64 * g + 64]).astype(BF)
            mixed = jnp.dot(mix, sig, preferred_element_type=F32) + upright(offs[g], 128)
            gated[b, :, 64 * g : 64 * g + 64] = (
                act_ref[at, 64 * g : 64 * g + 64] * mixed
            ).astype(BF)
    here = place[1]
    mine, other = gated[here], gated[1 - here]
    for block, half, ref, k in spread(order, pieces[:4], pieces[4:]):
        piece = ref[k, :, 384:576]
        cols = pl.ds(128 * half, 128)
        part = lax.dot_general(mine, piece, NT, preferred_element_type=F32)
        kept[block, :, cols] = part.astype(BF)
        part = lax.dot_general(other, piece, NT, preferred_element_type=F32)
        sent[block, :, cols] = part.astype(BF)


def exchange(own, flip):
    to_pair = [(i, (((i + flip) ^ 1) - flip) % 8) for i in range(8)]
    to_next = [(i, (((i + 1 - flip) ^ 1) - 1 + flip) % 8) for i in range(8)]
    got = lax.ppermute(own, "z", to_pair)
    batch = jnp.concatenate([own, got])
    pieces = [batch]
    for turn in (to_next, to_pair, to_next):
        batch = lax.ppermute(batch, "z", turn)
        pieces.append(batch)
    return pieces


def blocks(z):
    out = 2 * ((z + jnp.arange(2)) & 1) - 1
    steps = jnp.array([0, -1, 1, 2, -2, -3, 3, 4])
    return ((z + out[:, None] * steps) & 7).astype(jnp.int32)


def ffn_kernel(mid_ref, gain, w_ref, out_ref, w, acc, hid, sems):
    def fetch(n):
        part, k = divmod(n, 8)
        cols = pl.ds(1408 * part, 1408 - 704 * part)
        at = (k, slice(None), slice(None), slice(None), cols)
        return pltpu.make_async_copy(w_ref.at[at], w.at[at], sems.at[n])

    for n in range(8):
        fetch(n).start()

    def arrive(n):
        fetch(n).wait()
        if n < 8:
            fetch(n + 8).start()

    total = jnp.zeros((128, 1), F32)
    for k in range(8):
        v = mid_ref[k].astype(F32)
        total = total + jnp.sum(v * v, axis=1, keepdims=True)
    factor = lax.rsqrt(total / 2048.0 + EPS)
    for k in range(8):
        rows = (mid_ref[k].astype(F32) * factor * gain[k]).astype(BF)
        arrive(k)
        for c in range(2):
            piece = w[k, :, c, :, 0:1408].reshape(256, 1408)
            part = jnp.dot(rows, piece, preferred_element_type=F32)
            if k == 0:
                acc[c] = part
            else:
                acc[c] = acc[c] + part
    for c in range(2):
        g = acc[c, :, 0:640]
        u = acc[c, :, 640:1280]
        hid[c, :, 0:640] = (g * jax.nn.sigmoid(g) * u).astype(BF)
        g = acc[c, :, 1280:1344]
        u = acc[c, :, 1344:1408]
        hid[c, :, 640:704] = (g * jax.nn.sigmoid(g) * u).astype(BF)
    for k in range(8):
        if k % 4 == 0:
            for n in range(8 + k, 12 + k):
                arrive(n)
        part = jnp.zeros((128, 256), F32)
        for c in range(2):
            piece = w[k, :, c, :, 1408:2112].reshape(256, 704)
            part = part + lax.dot_general(hid[c], piece, NT, preferred_element_type=F32)
        out_ref[k] = part.astype(BF)


def on_device(
    sequence_entries,
    former_norm_factor,
    conveyor_matrix,
    conveyor_rescalers,
    blend_value_matrix,
    blend_rescalers,
    blend_norm_factor,
    location_matrices,
    location_offsets,
    branch_emission_matrix,
    emission_rescalers,
    latter_norm_factor,
    valve_matrix,
    valve_rescalers,
    raising_matrix,
    raising_rescalers,
    lowering_matrix,
    lowering_rescalers,
):
    z, x, c = lax.axis_index("z"), lax.axis_index("x"), lax.axis_index("c")
    swap = [(0, 1), (1, 0)]
    own = pl.pallas_call(
        pack_kernel,
        in_specs=[VM] * 4,
        out_specs=VM,
        out_shape=jax.ShapeDtypeStruct((8, 32, 640), BF),
        name="pack",
    )(conveyor_matrix, blend_value_matrix, branch_emission_matrix.T, emission_rescalers)
    ffn_own = pl.pallas_call(
        pack_ffn_kernel,
        in_specs=[VM] * 6,
        out_specs=VM,
        out_shape=jax.ShapeDtypeStruct((32, 2112), BF),
        name="pack_ffn",
    )(
        valve_matrix,
        valve_rescalers,
        raising_matrix,
        raising_rescalers,
        lowering_matrix.T,
        lowering_rescalers,
    )
    seqs, scales, gain, latter_gain, mats, offs, blend_gain = pl.pallas_call(
        keep_kernel,
        in_specs=[VM] * 8,
        out_specs=[VM] * 7,
        out_shape=[
            jax.ShapeDtypeStruct((8, 256, 256), BF),
            pltpu.VMEM((1, 384), F32),
            pltpu.VMEM((8, 1, 256), F32),
            pltpu.VMEM((8, 1, 256), F32),
            pltpu.VMEM((3, 128, 128), BF),
            pltpu.VMEM((3, 128), F32),
            pltpu.VMEM((1, 192), F32),
        ],
        name="keep",
    )(
        sequence_entries,
        conveyor_rescalers,
        blend_rescalers,
        former_norm_factor.reshape(8, 1, 256),
        latter_norm_factor.reshape(8, 1, 256),
        location_matrices,
        location_offsets,
        blend_norm_factor.reshape(1, 192),
    )
    ffn_all = lax.all_gather(ffn_own, ("z", "y", "c"), axis=0, tiled=True)

    first = lax.all_to_all(own, "y", 0, 0, tiled=True)
    rows = lax.all_to_all(seqs, TP, 0, 0, tiled=True)
    left = [vmem(p) for p in exchange(first[:4].reshape(1, 128, 640), 0)]
    right = [vmem(p) for p in exchange(first[4:].reshape(1, 128, 640), 1)]
    pieces = left + right
    order = blocks(z)
    near = vmem(rows)

    prior, factor = pl.pallas_call(
        early_kernel,
        in_specs=[SM] + [VM] * 8,
        out_specs=[VM, VM],
        out_shape=[pltpu.VMEM((256, 384), F32), pltpu.VMEM((256, 128), F32)],
        compiler_params=limit(4),
        name="early",
    )(order, near, gain, *left[:3], *right[:3])
    here = jnp.stack([x, c]).astype(jnp.int32)
    act, own_sq, base = pl.pallas_call(
        project_kernel,
        in_specs=[SM, SM] + [VM] * 7,
        out_specs=[VM] * 3,
        out_shape=[
            pltpu.VMEM((256, 384), F32),
            jax.ShapeDtypeStruct((8, 1, 256), F32),
            jax.ShapeDtypeStruct((2, 128, 256), BF),
        ],
        compiler_params=limit(4),
        name="project",
    )(order, here, near, gain, scales, prior, factor, left[3], right[3])
    all_sq = lax.all_to_all(own_sq, TP, 0, 0, tiled=True)
    kept, sent = pl.pallas_call(
        gate_kernel,
        in_specs=[SM, SM] + [VM] * 13,
        out_specs=[VM, VM],
        out_shape=[jax.ShapeDtypeStruct((8, 128, 256), BF)] * 2,
        scratch_shapes=[pltpu.VMEM((2, 128, 192), BF)],
        compiler_params=limit(6),
        name="gating",
    )(
        order,
        here,
        act,
        all_sq,
        mats,
        offs,
        blend_gain,
        *pieces,
    )
    got = lax.ppermute(sent, "c", swap)
    both = (kept.astype(F32) + got.astype(F32)).astype(BF).reshape(4, 2, 128, 256)
    shares = lax.all_to_all(both, "x", 0, 0, tiled=True)
    mid_own = (base.astype(F32) + jnp.sum(shares.astype(F32), axis=0)).astype(BF)
    mid = from_everyone(mid_own, "x").reshape(8, 128, 256)
    outs = pl.pallas_call(
        ffn_kernel,
        in_specs=[VM, VM, pl.BlockSpec(memory_space=pltpu.HBM)],
        out_specs=VM,
        out_shape=jax.ShapeDtypeStruct((8, 128, 256), BF),
        scratch_shapes=[
            pltpu.VMEM((8, 8, 2, 32, 2112), BF),
            pltpu.VMEM((2, 128, 1408), F32),
            pltpu.VMEM((2, 128, 704), BF),
            pltpu.SemaphoreType.DMA((16,)),
        ],
        name="ffn",
    )(vmem(mid), latter_gain, ffn_all.reshape(8, 8, 2, 32, 2112))
    ffn_shares = lax.all_to_all(outs, TP, 0, 0, tiled=True).reshape(4, 2, 128, 256)
    mid_kept = lax.dynamic_index_in_dim(mid_own, c, 0, keepdims=False)
    mid_sent = lax.dynamic_index_in_dim(mid_own, 1 - c, 0, keepdims=False)
    mid_got = lax.ppermute(mid_sent, "c", swap)
    lower = jnp.where(c == 0, mid_kept, mid_got)
    upper = jnp.where(c == 0, mid_got, mid_kept)
    mid_here = jnp.stack([lower, upper])
    out = mid_here.astype(F32) + jnp.sum(ffn_shares.astype(F32), axis=0)
    return out.astype(BF).reshape(256, 256)


def limit(mib):
    return pltpu.CompilerParams(vmem_limit_bytes=mib << 20)


def vmem(x):
    return pltpu.with_memory_space_constraint(x, pltpu.VMEM)


def solution(mesh):
    finer = Mesh(mesh.devices.reshape(8, 8, 4, 2), ("z", "y", "x", "c"))
    return jax.shard_map(
        on_device,
        mesh=finer,
        in_specs=(
            P(FS, TP),
            P(),
            P(FS, TP),
            P(TP),
            P(FS, TP),
            P(TP),
            P(TP),
            P(TP, None, None),
            P(TP, None),
            P(TP, FS),
            P(FS),
            P(),
            P(FS, TP),
            P(TP),
            P(FS, TP),
            P(TP),
            P(TP, FS),
            P(FS),
        ),
        out_specs=P(FS, TP),
        check_vma=False,
    )
```

```python
import jax
import jax.numpy as jnp
from jax import lax
from jax.experimental import pallas as pl
from jax.experimental.pallas import tpu as pltpu
from jax.sharding import Mesh
from jax.sharding import PartitionSpec as P

FS = ("z", "y")
TP = ("x", "c")
EPS = 1e-06
BF = jnp.bfloat16
F32 = jnp.float32
NT = (((1,), (1,)), ((), ()))
VM = pl.BlockSpec(memory_space=pltpu.VMEM)
SM = pl.BlockSpec(memory_space=pltpu.SMEM)
ANY = pl.BlockSpec(memory_space=pl.ANY)


def from_everyone(x, axis):
    copies = jnp.broadcast_to(x, (lax.axis_size(axis), *x.shape))
    return lax.all_to_all(copies, axis, split_axis=0, concat_axis=0, tiled=True)


def gelu(v):
    return 0.5 * v * (1.0 + jnp.tanh(0.7978845608028654 * (v + 0.044715 * v * v * v)))


def upright(row, n):
    same = lax.broadcasted_iota(jnp.int32, (n, n), 0) == lax.broadcasted_iota(jnp.int32, (n, n), 1)
    return jnp.sum(jnp.where(same, row.reshape(1, n), 0.0), axis=1, keepdims=True)


def pack_kernel(conv, blend, emis, emis_s, own):
    emission = emis[...] * upright(emis_s[...], 32)
    packed = jnp.concatenate([conv[...], blend[...], emission, jnp.zeros((32, 64), F32)], axis=1)
    packed = packed.astype(BF)
    for k in range(8):
        own[k] = packed


def pack_ffn_kernel(valve, valve_s, raising, raising_s, low, low_s, ffn):
    gate = valve[...] * valve_s[...].reshape(1, 704)
    up = raising[...] * raising_s[...].reshape(1, 704)
    ffn[:, 0:640] = gate[:, 0:640].astype(BF)
    ffn[:, 640:1280] = up[:, 0:640].astype(BF)
    ffn[:, 1280:1408] = jnp.concatenate([gate[:, 640:704], up[:, 640:704]], axis=1).astype(BF)
    ffn[:, 1408:2112] = (low[...] * upright(low_s[...], 32)).astype(BF)


def keep_kernel(seq, conv_s, blend_s, gain1, gain2, mats, offs, blend_gain, seqs, scales, keep1, keep2, group):
    for k in range(8):
        seqs[k] = seq[...]
    scales[:, 0:192] = conv_s[...].reshape(1, 192)
    scales[:, 192:384] = blend_s[...].reshape(1, 192)
    keep1[...] = gain1[...]
    keep2[...] = gain2[...]
    for g in range(3):
        group[128 * g : 128 * g + 128] = mats[g].astype(F32)
    group[384:387] = offs[...]
    gains = blend_gain[...]
    for g in range(3):
        group[392 + g : 393 + g, 0:64] = gains[:, 64 * g : 64 * g + 64]
        group[392 + g : 393 + g, 64:128] = jnp.zeros((1, 64), F32)
    group[387:392] = jnp.zeros((5, 128), F32)
    group[395:400] = jnp.zeros((5, 128), F32)


def spread(order, left, right, place=0):
    found = []
    for half, refs in enumerate((left, right)):
        at = place
        for ref in refs:
            for k in range(ref.shape[0]):
                found.append((order[half, at], half, ref, k))
                at += 1
    return found


def multiply(found, x_ref, gain, factor, prior):
    for block, half, ref, k in found:
        cols = pl.ds(128 * half, 128)
        rows = (x_ref[block, :, cols].astype(F32) * factor * gain[block, :, cols]).astype(BF)
        prior = prior + jnp.dot(rows, ref[k, :, 0:384], preferred_element_type=F32)
    return prior


def early_kernel(order, x_ref, gain, *refs):
    pieces, prior_ref, factor_ref = refs[:6], refs[6], refs[7]
    total = jnp.zeros((256, 1), F32)
    for k in range(8):
        v = x_ref[k].astype(F32)
        total = total + jnp.sum(v * v, axis=1, keepdims=True)
    factor = lax.rsqrt(total / 2048.0 + EPS)
    factor_ref[...] = jnp.broadcast_to(factor, (256, 128))
    found = spread(order, pieces[:3], pieces[3:])
    prior_ref[...] = multiply(found, x_ref, gain, factor, jnp.zeros((256, 384), F32))


def project_kernel(order, here, x_ref, gain, scales, prior, factor, *refs):
    pieces, (mine, yours, sq_ref, base, emis) = refs[:8], refs[8:]
    base[...] = x_ref[pl.ds(2 * here[0], 2), pl.ds(pl.multiple_of(128 * here[1], 128), 128), :]
    for block, half, ref, k in spread(order, pieces[:4], pieces[4:]):
        emis[block, pl.ds(128 * half, 128), :] = ref[k, :, 384:640]
    found = spread(order, pieces[3:4], pieces[7:8], 6)
    sums = multiply(found, x_ref, gain, factor[:, 0:1], prior[...])
    act = gelu(sums * scales[...])
    first = here[1] == 0
    mine[...] = jnp.where(first, act[0:128], act[128:256])
    yours[...] = jnp.where(first, act[128:256], act[0:128])
    signal = act[:, 192:384]
    ones = jnp.ones((8, 192), F32)
    squares = lax.dot_general(
        ones, signal * signal, NT, precision=lax.Precision.HIGHEST, preferred_element_type=F32
    )
    sq_ref[...] = jnp.broadcast_to(squares[0:1].reshape(1, 1, 256), (8, 1, 256))


def gate_kernel(place, mine, theirs, sq_ref, my_group, their_group, my_emis, their_emis, out_ref, gated):
    total = jnp.sum(sq_ref[...], axis=0)
    factor = lax.rsqrt(total / 1536.0 + EPS)
    factor = jnp.where(place[1] == 0, factor[:, 0:128], factor[:, 128:256])
    rows = lax.broadcasted_iota(jnp.int32, (128, 128), 0)
    cols = lax.broadcasted_iota(jnp.int32, (128, 128), 1)
    lower = cols <= rows
    for side, (act, group) in enumerate(((mine, my_group), (theirs, their_group))):
        for g in range(3):
            mat = jnp.where(lower, group[128 * g : 128 * g + 128], 0.0)
            mix = (mat * factor).astype(BF)
            gains = group[392 + g : 393 + g, 0:64]
            sig = (act[:, 192 + 64 * g : 256 + 64 * g] * gains).astype(BF)
            mixed = jnp.dot(mix, sig, preferred_element_type=F32) + upright(group[384 + g], 128)
            gated[side, :, 64 * g : 64 * g + 64] = (act[:, 64 * g : 64 * g + 64] * mixed).astype(BF)
    for k in range(8):
        part = lax.dot_general(gated[0], my_emis[k, :, 0:192], NT, preferred_element_type=F32)
        more = lax.dot_general(gated[1], their_emis[k, :, 0:192], NT, preferred_element_type=F32)
        out_ref[k] = (part + more).astype(BF)


def exchange(own, flip):
    to_pair = [(i, (((i + flip) ^ 1) - flip) % 8) for i in range(8)]
    to_next = [(i, (((i + 1 - flip) ^ 1) - 1 + flip) % 8) for i in range(8)]
    got = lax.ppermute(own, "z", to_pair)
    batch = jnp.concatenate([own, got])
    pieces = [batch]
    for turn in (to_next, to_pair, to_next):
        batch = lax.ppermute(batch, "z", turn)
        pieces.append(batch)
    return pieces


def blocks(z):
    out = 2 * ((z + jnp.arange(2)) & 1) - 1
    steps = jnp.array([0, -1, 1, 2, -2, -3, 3, 4])
    return ((z + out[:, None] * steps) & 7).astype(jnp.int32)


def ffn_kernel(mid_ref, gain, w_ref, out_ref, w, acc, hid, sems):
    def fetch(n):
        part, k = divmod(n, 8)
        cols = pl.ds(1408 * part, 1408 - 704 * part)
        at = (k, slice(None), slice(None), slice(None), cols)
        return pltpu.make_async_copy(w_ref.at[at], w.at[at], sems.at[n])

    for n in range(8):
        fetch(n).start()

    def arrive(n):
        fetch(n).wait()
        if n < 8:
            fetch(n + 8).start()

    total = jnp.zeros((128, 1), F32)
    for k in range(8):
        v = mid_ref[k].astype(F32)
        total = total + jnp.sum(v * v, axis=1, keepdims=True)
    factor = lax.rsqrt(total / 2048.0 + EPS)
    for k in range(8):
        rows = (mid_ref[k].astype(F32) * factor * gain[k]).astype(BF)
        arrive(k)
        for c in range(2):
            piece = w[k, :, c, :, 0:1408].reshape(256, 1408)
            part = jnp.dot(rows, piece, preferred_element_type=F32)
            if k == 0:
                acc[c] = part
            else:
                acc[c] = acc[c] + part
    for c in range(2):
        g = acc[c, :, 0:640]
        u = acc[c, :, 640:1280]
        hid[c, :, 0:640] = (g * jax.nn.sigmoid(g) * u).astype(BF)
        g = acc[c, :, 1280:1344]
        u = acc[c, :, 1344:1408]
        hid[c, :, 640:704] = (g * jax.nn.sigmoid(g) * u).astype(BF)
    for k in range(8):
        if k % 4 == 0:
            for n in range(8 + k, 12 + k):
                arrive(n)
        part = jnp.zeros((128, 256), F32)
        for c in range(2):
            piece = w[k, :, c, :, 1408:2112].reshape(256, 704)
            part = part + lax.dot_general(hid[c], piece, NT, preferred_element_type=F32)
        out_ref[k] = part.astype(BF)


def on_device(
    sequence_entries,
    former_norm_factor,
    conveyor_matrix,
    conveyor_rescalers,
    blend_value_matrix,
    blend_rescalers,
    blend_norm_factor,
    location_matrices,
    location_offsets,
    branch_emission_matrix,
    emission_rescalers,
    latter_norm_factor,
    valve_matrix,
    valve_rescalers,
    raising_matrix,
    raising_rescalers,
    lowering_matrix,
    lowering_rescalers,
):
    z, x, c = lax.axis_index("z"), lax.axis_index("x"), lax.axis_index("c")
    swap = [(0, 1), (1, 0)]
    own = pl.pallas_call(
        pack_kernel,
        in_specs=[VM] * 4,
        out_specs=VM,
        out_shape=jax.ShapeDtypeStruct((8, 32, 640), BF),
        name="pack",
    )(conveyor_matrix, blend_value_matrix, branch_emission_matrix.T, emission_rescalers)
    ffn_own = pl.pallas_call(
        pack_ffn_kernel,
        in_specs=[VM] * 6,
        out_specs=VM,
        out_shape=jax.ShapeDtypeStruct((32, 2112), BF),
        name="pack_ffn",
    )(
        valve_matrix,
        valve_rescalers,
        raising_matrix,
        raising_rescalers,
        lowering_matrix.T,
        lowering_rescalers,
    )
    seqs, scales, gain, latter_gain, group = pl.pallas_call(
        keep_kernel,
        in_specs=[VM] * 8,
        out_specs=[VM] * 5,
        out_shape=[
            jax.ShapeDtypeStruct((8, 256, 256), BF),
            pltpu.VMEM((1, 384), F32),
            pltpu.VMEM((8, 1, 256), F32),
            pltpu.VMEM((8, 1, 256), F32),
            jax.ShapeDtypeStruct((400, 128), F32),
        ],
        name="keep",
    )(
        sequence_entries,
        conveyor_rescalers,
        blend_rescalers,
        former_norm_factor.reshape(8, 1, 256),
        latter_norm_factor.reshape(8, 1, 256),
        location_matrices,
        location_offsets,
        blend_norm_factor.reshape(1, 192),
    )
    other_group = lax.ppermute(group, "c", swap)
    ffn_all = lax.all_gather(ffn_own, ("z", "y", "c"), axis=0, tiled=True)

    first = lax.all_to_all(own, "y", 0, 0, tiled=True)
    rows = lax.all_to_all(seqs, TP, 0, 0, tiled=True)
    left = [vmem(p) for p in exchange(first[:4].reshape(1, 128, 640), 0)]
    right = [vmem(p) for p in exchange(first[4:].reshape(1, 128, 640), 1)]
    order = blocks(z)
    near = vmem(rows)

    prior, factor = pl.pallas_call(
        early_kernel,
        in_specs=[SM] + [VM] * 8,
        out_specs=[VM, VM],
        out_shape=[pltpu.VMEM((256, 384), F32), pltpu.VMEM((256, 128), F32)],
        compiler_params=limit(4),
        name="early",
    )(order, near, gain, *left[:3], *right[:3])
    here = jnp.stack([x, c]).astype(jnp.int32)
    mine, yours, own_sq, base, emis = pl.pallas_call(
        project_kernel,
        in_specs=[SM, SM] + [VM] * 13,
        out_specs=[VM] * 5,
        out_shape=[
            jax.ShapeDtypeStruct((128, 384), F32),
            jax.ShapeDtypeStruct((128, 384), F32),
            jax.ShapeDtypeStruct((8, 1, 256), F32),
            jax.ShapeDtypeStruct((2, 128, 256), BF),
            jax.ShapeDtypeStruct((8, 256, 256), BF),
        ],
        compiler_params=limit(52),
        name="project",
    )(order, here, near, gain, scales, prior, factor, *left, *right)
    all_sq = lax.all_to_all(own_sq, TP, 0, 0, tiled=True)
    theirs = lax.ppermute(yours, "c", swap)
    other_emis = lax.ppermute(emis, "c", swap)
    both = pl.pallas_call(
        gate_kernel,
        in_specs=[SM] + [VM] * 7,
        out_specs=VM,
        out_shape=jax.ShapeDtypeStruct((8, 128, 256), BF),
        scratch_shapes=[pltpu.VMEM((2, 128, 192), BF)],
        name="gating",
    )(here, mine, theirs, all_sq, group, other_group, emis, other_emis)
    both = both.reshape(4, 2, 128, 256)
    shares = lax.all_to_all(both, "x", 0, 0, tiled=True)
    mid_own = (base.astype(F32) + jnp.sum(shares.astype(F32), axis=0)).astype(BF)
    mid = from_everyone(mid_own, "x").reshape(8, 128, 256)
    outs = pl.pallas_call(
        ffn_kernel,
        in_specs=[VM, VM, pl.BlockSpec(memory_space=pltpu.HBM)],
        out_specs=VM,
        out_shape=jax.ShapeDtypeStruct((8, 128, 256), BF),
        scratch_shapes=[
            pltpu.VMEM((8, 8, 2, 32, 2112), BF),
            pltpu.VMEM((2, 128, 1408), F32),
            pltpu.VMEM((2, 128, 704), BF),
            pltpu.SemaphoreType.DMA((16,)),
        ],
        name="ffn",
    )(vmem(mid), latter_gain, ffn_all.reshape(8, 8, 2, 32, 2112))
    ffn_shares = lax.all_to_all(outs, TP, 0, 0, tiled=True).reshape(4, 2, 128, 256)
    mid_kept = lax.dynamic_index_in_dim(mid_own, c, 0, keepdims=False)
    mid_sent = lax.dynamic_index_in_dim(mid_own, 1 - c, 0, keepdims=False)
    mid_got = lax.ppermute(mid_sent, "c", swap)
    lower = jnp.where(c == 0, mid_kept, mid_got)
    upper = jnp.where(c == 0, mid_got, mid_kept)
    mid_here = jnp.stack([lower, upper])
    out = mid_here.astype(F32) + jnp.sum(ffn_shares.astype(F32), axis=0)
    return out.astype(BF).reshape(256, 256)


def limit(mib):
    return pltpu.CompilerParams(vmem_limit_bytes=mib << 20)


def vmem(x):
    return pltpu.with_memory_space_constraint(x, pltpu.VMEM)


def solution(mesh):
    finer = Mesh(mesh.devices.reshape(8, 8, 4, 2), ("z", "y", "x", "c"))
    return jax.shard_map(
        on_device,
        mesh=finer,
        in_specs=(
            P(FS, TP),
            P(),
            P(FS, TP),
            P(TP),
            P(FS, TP),
            P(TP),
            P(TP),
            P(TP, None, None),
            P(TP, None),
            P(TP, FS),
            P(FS),
            P(),
            P(FS, TP),
            P(TP),
            P(FS, TP),
            P(TP),
            P(TP, FS),
            P(FS),
        ),
        out_specs=P(FS, TP),
        check_vma=False,
    )
```

```python
import jax
import jax.numpy as jnp
from jax import lax
from jax.experimental import pallas as pl
from jax.experimental.pallas import tpu as pltpu
from jax.sharding import Mesh
from jax.sharding import PartitionSpec as P

FS = ("z", "y")
TP = ("x", "c")
EPS = 1e-06
BF = jnp.bfloat16
F32 = jnp.float32
NT = (((1,), (1,)), ((), ()))
VM = pl.BlockSpec(memory_space=pltpu.VMEM)
SM = pl.BlockSpec(memory_space=pltpu.SMEM)
ANY = pl.BlockSpec(memory_space=pl.ANY)


def from_everyone(x, axis):
    copies = jnp.broadcast_to(x, (lax.axis_size(axis), *x.shape))
    return lax.all_to_all(copies, axis, split_axis=0, concat_axis=0, tiled=True)


def gelu(v):
    return 0.5 * v * (1.0 + jnp.tanh(0.7978845608028654 * (v + 0.044715 * v * v * v)))


def upright(row, n):
    same = lax.broadcasted_iota(jnp.int32, (n, n), 0) == lax.broadcasted_iota(jnp.int32, (n, n), 1)
    return jnp.sum(jnp.where(same, row.reshape(1, n), 0.0), axis=1, keepdims=True)


def pack_kernel(conv, blend, emis, emis_s, own):
    emission = emis[...] * upright(emis_s[...], 32)
    packed = jnp.concatenate([conv[...], blend[...], emission, jnp.zeros((32, 64), F32)], axis=1)
    packed = packed.astype(BF)
    for k in range(8):
        own[k] = packed


def pack_later_kernel(valve, valve_s, raising, raising_s, low, low_s, seq, *refs):
    ffn, seqs, scales = refs[7:10]
    scales[:, 0:192] = refs[0][...].reshape(1, 192)
    scales[:, 192:384] = refs[1][...].reshape(1, 192)
    for here, there in zip(refs[2:7], refs[10:]):
        there[...] = here[...]
    for k in range(8):
        seqs[k] = seq[...]
    gate = valve[...] * valve_s[...].reshape(1, 704)
    up = raising[...] * raising_s[...].reshape(1, 704)
    ffn[:, 0:640] = gate[:, 0:640].astype(BF)
    ffn[:, 640:1280] = up[:, 0:640].astype(BF)
    ffn[:, 1280:1408] = jnp.concatenate([gate[:, 640:704], up[:, 640:704]], axis=1).astype(BF)
    ffn[:, 1408:2112] = (low[...] * upright(low_s[...], 32)).astype(BF)


def spread(order, left, right, place=0):
    found = []
    for half, refs in enumerate((left, right)):
        at = place
        for ref in refs:
            for k in range(ref.shape[0]):
                found.append((order[half, at], half, ref, k))
                at += 1
    return found


def multiply(found, x_ref, gain, factor, prior):
    for block, half, ref, k in found:
        cols = pl.ds(128 * half, 128)
        rows = (x_ref[block, :, cols].astype(F32) * factor * gain[block, :, cols]).astype(BF)
        prior = prior + jnp.dot(rows, ref[k, :, 0:384], preferred_element_type=F32)
    return prior


def early_kernel(order, x_ref, gain, *refs):
    pieces, prior_ref, factor_ref = refs[:6], refs[6], refs[7]
    total = jnp.zeros((256, 1), F32)
    for k in range(8):
        v = x_ref[k].astype(F32)
        total = total + jnp.sum(v * v, axis=1, keepdims=True)
    factor = lax.rsqrt(total / 2048.0 + EPS)
    factor_ref[...] = jnp.broadcast_to(factor, (256, 128))
    found = spread(order, pieces[:3], pieces[3:])
    prior_ref[...] = multiply(found, x_ref, gain, factor, jnp.zeros((256, 384), F32))


def project_kernel(order, here, x_ref, gain, scales, prior, factor, left, right, act_ref, sq_ref, base):
    base[...] = x_ref[pl.ds(2 * here[0], 2), pl.ds(pl.multiple_of(128 * here[1], 128), 128), :]
    found = spread(order, [left], [right], 6)
    prior = multiply(found, x_ref, gain, factor[:, 0:1], prior[...])
    act = gelu(prior * scales[...])
    act_ref[...] = act
    signal = act[:, 192:384]
    ones = jnp.ones((8, 192), F32)
    sums = lax.dot_general(
        ones, signal * signal, NT, precision=lax.Precision.HIGHEST, preferred_element_type=F32
    )
    sq_ref[...] = jnp.broadcast_to(sums[0:1].reshape(1, 1, 256), (8, 1, 256))


def gate_kernel(order, place, act_ref, sq_ref, mats, offs, gain, *refs):
    pieces, kept, sent, gated = refs[:8], refs[8], refs[9], refs[10]
    total = jnp.sum(sq_ref[...], axis=0)
    factor = lax.rsqrt(total / 1536.0 + EPS)
    rows = lax.broadcasted_iota(jnp.int32, (128, 128), 0)
    cols = lax.broadcasted_iota(jnp.int32, (128, 128), 1)
    lower = cols <= rows
    gains = gain[...]
    for g in range(3):
        mat = jnp.where(lower, mats[g].astype(F32), 0.0)
        for b in range(2):
            at = pl.ds(128 * b, 128)
            mix = (mat * factor[:, 128 * b : 128 * b + 128]).astype(BF)
            sig = (act_ref[at, 192 + 64 * g : 256 + 64 * g] * gains[:, 64 * g : 64 * g + 64]).astype(BF)
            mixed = jnp.dot(mix, sig, preferred_element_type=F32) + upright(offs[g], 128)
            gated[b, :, 64 * g : 64 * g + 64] = (
                act_ref[at, 64 * g : 64 * g + 64] * mixed
            ).astype(BF)
    here = place[1]
    mine, other = gated[here], gated[1 - here]
    for block, half, ref, k in spread(order, pieces[:4], pieces[4:]):
        piece = ref[k, :, 384:576]
        cols = pl.ds(128 * half, 128)
        part = lax.dot_general(mine, piece, NT, preferred_element_type=F32)
        kept[block, :, cols] = part.astype(BF)
        part = lax.dot_general(other, piece, NT, preferred_element_type=F32)
        sent[block, :, cols] = part.astype(BF)


def exchange(own, flip):
    to_pair = [(i, (((i + flip) ^ 1) - flip) % 8) for i in range(8)]
    to_next = [(i, (((i + 1 - flip) ^ 1) - 1 + flip) % 8) for i in range(8)]
    got = lax.ppermute(own, "z", to_pair)
    batch = jnp.concatenate([own, got])
    pieces = [batch]
    for turn in (to_next, to_pair, to_next):
        batch = lax.ppermute(batch, "z", turn)
        pieces.append(batch)
    return pieces


def blocks(z):
    out = 2 * ((z + jnp.arange(2)) & 1) - 1
    steps = jnp.array([0, -1, 1, 2, -2, -3, 3, 4])
    return ((z + out[:, None] * steps) & 7).astype(jnp.int32)


def ffn_kernel(mid_ref, gain, w_ref, out_ref, w, acc, hid, sems):
    def fetch(n):
        part, k = divmod(n, 8)
        cols = pl.ds(1408 * part, 1408 - 704 * part)
        at = (k, slice(None), slice(None), slice(None), cols)
        return pltpu.make_async_copy(w_ref.at[at], w.at[at], sems.at[n])

    for n in range(8):
        fetch(n).start()

    def arrive(n):
        fetch(n).wait()
        if n < 8:
            fetch(n + 8).start()

    total = jnp.zeros((128, 1), F32)
    for k in range(8):
        v = mid_ref[k].astype(F32)
        total = total + jnp.sum(v * v, axis=1, keepdims=True)
    factor = lax.rsqrt(total / 2048.0 + EPS)
    for k in range(8):
        rows = (mid_ref[k].astype(F32) * factor * gain[k]).astype(BF)
        arrive(k)
        for c in range(2):
            piece = w[k, :, c, :, 0:1408].reshape(256, 1408)
            part = jnp.dot(rows, piece, preferred_element_type=F32)
            if k == 0:
                acc[c] = part
            else:
                acc[c] = acc[c] + part
    for c in range(2):
        g = acc[c, :, 0:640]
        u = acc[c, :, 640:1280]
        hid[c, :, 0:640] = (g * jax.nn.sigmoid(g) * u).astype(BF)
        g = acc[c, :, 1280:1344]
        u = acc[c, :, 1344:1408]
        hid[c, :, 640:704] = (g * jax.nn.sigmoid(g) * u).astype(BF)
    for k in range(8):
        if k % 4 == 0:
            for n in range(8 + k, 12 + k):
                arrive(n)
        part = jnp.zeros((128, 256), F32)
        for c in range(2):
            piece = w[k, :, c, :, 1408:2112].reshape(256, 704)
            part = part + lax.dot_general(hid[c], piece, NT, preferred_element_type=F32)
        out_ref[k] = part.astype(BF)


def on_device(
    sequence_entries,
    former_norm_factor,
    conveyor_matrix,
    conveyor_rescalers,
    blend_value_matrix,
    blend_rescalers,
    blend_norm_factor,
    location_matrices,
    location_offsets,
    branch_emission_matrix,
    emission_rescalers,
    latter_norm_factor,
    valve_matrix,
    valve_rescalers,
    raising_matrix,
    raising_rescalers,
    lowering_matrix,
    lowering_rescalers,
):
    z, x, c = lax.axis_index("z"), lax.axis_index("x"), lax.axis_index("c")
    swap = [(0, 1), (1, 0)]
    own = pl.pallas_call(
        pack_kernel,
        in_specs=[VM] * 4,
        out_specs=VM,
        out_shape=jax.ShapeDtypeStruct((8, 32, 640), BF),
        name="pack",
    )(conveyor_matrix, blend_value_matrix, branch_emission_matrix.T, emission_rescalers)
    ffn_own, seqs, scales, gain, latter_gain, mats, offs, blend_gain = pl.pallas_call(
        pack_later_kernel,
        in_specs=[VM] * 14,
        out_specs=[VM] * 8,
        out_shape=[
            jax.ShapeDtypeStruct((32, 2112), BF),
            jax.ShapeDtypeStruct((8, 256, 256), BF),
            pltpu.VMEM((1, 384), F32),
            pltpu.VMEM((8, 1, 256), F32),
            pltpu.VMEM((8, 1, 256), F32),
            pltpu.VMEM((3, 128, 128), BF),
            pltpu.VMEM((3, 128), F32),
            pltpu.VMEM((1, 192), F32),
        ],
        name="pack_later",
    )(
        valve_matrix,
        valve_rescalers,
        raising_matrix,
        raising_rescalers,
        lowering_matrix.T,
        lowering_rescalers,
        sequence_entries,
        conveyor_rescalers,
        blend_rescalers,
        former_norm_factor.reshape(8, 1, 256),
        latter_norm_factor.reshape(8, 1, 256),
        location_matrices,
        location_offsets,
        blend_norm_factor.reshape(1, 192),
    )
    ffn_all = lax.all_gather(ffn_own, ("z", "y", "c"), axis=0, tiled=True)

    first = lax.all_to_all(own, "y", 0, 0, tiled=True)
    rows = lax.all_to_all(seqs, TP, 0, 0, tiled=True)
    left = [vmem(p) for p in exchange(first[:4].reshape(1, 128, 640), 0)]
    right = [vmem(p) for p in exchange(first[4:].reshape(1, 128, 640), 1)]
    pieces = left + right
    order = blocks(z)
    near = vmem(rows)

    prior, factor = pl.pallas_call(
        early_kernel,
        in_specs=[SM] + [VM] * 8,
        out_specs=[VM, VM],
        out_shape=[pltpu.VMEM((256, 384), F32), pltpu.VMEM((256, 128), F32)],
        compiler_params=limit(4),
        name="early",
    )(order, near, gain, *left[:3], *right[:3])
    here = jnp.stack([x, c]).astype(jnp.int32)
    act, own_sq, base = pl.pallas_call(
        project_kernel,
        in_specs=[SM, SM] + [VM] * 7,
        out_specs=[VM] * 3,
        out_shape=[
            pltpu.VMEM((256, 384), F32),
            jax.ShapeDtypeStruct((8, 1, 256), F32),
            jax.ShapeDtypeStruct((2, 128, 256), BF),
        ],
        compiler_params=limit(4),
        name="project",
    )(order, here, near, gain, scales, prior, factor, left[3], right[3])
    all_sq = lax.all_to_all(own_sq, TP, 0, 0, tiled=True)
    kept, sent = pl.pallas_call(
        gate_kernel,
        in_specs=[SM, SM] + [VM] * 13,
        out_specs=[VM, VM],
        out_shape=[jax.ShapeDtypeStruct((8, 128, 256), BF)] * 2,
        scratch_shapes=[pltpu.VMEM((2, 128, 192), BF)],
        compiler_params=limit(6),
        name="gating",
    )(
        order,
        here,
        act,
        all_sq,
        mats,
        offs,
        blend_gain,
        *pieces,
    )
    got = lax.ppermute(sent, "c", swap)
    both = (kept.astype(F32) + got.astype(F32)).astype(BF).reshape(4, 2, 128, 256)
    shares = lax.all_to_all(both, "x", 0, 0, tiled=True)
    mid_own = (base.astype(F32) + jnp.sum(shares.astype(F32), axis=0)).astype(BF)
    mid = from_everyone(mid_own, "x").reshape(8, 128, 256)
    outs = pl.pallas_call(
        ffn_kernel,
        in_specs=[VM, VM, pl.BlockSpec(memory_space=pltpu.HBM)],
        out_specs=VM,
        out_shape=jax.ShapeDtypeStruct((8, 128, 256), BF),
        scratch_shapes=[
            pltpu.VMEM((8, 8, 2, 32, 2112), BF),
            pltpu.VMEM((2, 128, 1408), F32),
            pltpu.VMEM((2, 128, 704), BF),
            pltpu.SemaphoreType.DMA((16,)),
        ],
        name="ffn",
    )(vmem(mid), latter_gain, ffn_all.reshape(8, 8, 2, 32, 2112))
    ffn_shares = lax.all_to_all(outs, TP, 0, 0, tiled=True).reshape(4, 2, 128, 256)
    mid_kept = lax.dynamic_index_in_dim(mid_own, c, 0, keepdims=False)
    mid_sent = lax.dynamic_index_in_dim(mid_own, 1 - c, 0, keepdims=False)
    mid_got = lax.ppermute(mid_sent, "c", swap)
    lower = jnp.where(c == 0, mid_kept, mid_got)
    upper = jnp.where(c == 0, mid_got, mid_kept)
    mid_here = jnp.stack([lower, upper])
    out = mid_here.astype(F32) + jnp.sum(ffn_shares.astype(F32), axis=0)
    return out.astype(BF).reshape(256, 256)


def limit(mib):
    return pltpu.CompilerParams(vmem_limit_bytes=mib << 20)


def vmem(x):
    return pltpu.with_memory_space_constraint(x, pltpu.VMEM)


def solution(mesh):
    finer = Mesh(mesh.devices.reshape(8, 8, 4, 2), ("z", "y", "x", "c"))
    return jax.shard_map(
        on_device,
        mesh=finer,
        in_specs=(
            P(FS, TP),
            P(),
            P(FS, TP),
            P(TP),
            P(FS, TP),
            P(TP),
            P(TP),
            P(TP, None, None),
            P(TP, None),
            P(TP, FS),
            P(FS),
            P(),
            P(FS, TP),
            P(TP),
            P(FS, TP),
            P(TP),
            P(TP, FS),
            P(FS),
        ),
        out_specs=P(FS, TP),
        check_vma=False,
    )
```
